256 devices in a mesh: fs: 64 (over z, x, core), tp: 4 (over y).
Axes of the slice: x: 4, y: 4, z: 8, core: 2. Of those that a mesh axis runs over, the one named last changes fastest.
Arguments:
- x_late: bfloat16 [32768, 2048], P(('fs', 'tp')), may hold values from -6 to 6
- x_early: bfloat16 [32768, 2048], P(('fs', 'tp')), may hold values from -24 to 24
- d_hidden: bfloat16 [32768, 3072], P('fs', 'tp'), may hold values from -16 to 16
- w_gate: bfloat16 [2048, 3072], P('fs', 'tp'), may hold values from -0.125 to 0.125
- w_up: bfloat16 [2048, 3072], P('fs', 'tp'), may hold values from -0.125 to 0.125
- gate_sum: float32 [2048, 3072], P('fs', 'tp'), may hold values from -512 to 512
- up_sum: float32 [2048, 3072], P('fs', 'tp'), may hold values from -512 to 512
Outputs:
- hidden_late: bfloat16 [32768, 3072], P('fs', 'tp')
- grad_input: bfloat16 [32768, 2048], P(('fs', 'tp'))
- gate_sum_out: float32 [2048, 3072], P('fs', 'tp')
- up_sum_out: float32 [2048, 3072], P('fs', 'tp')
The draws below stay inside these ranges and needn't reach their ends.
All inputs are finite; a program needn't handle non-finite values.
Results may differ from the reference program's by a relative error of at most 0.0095.
Values may be sent and summed in bfloat16 or wider, within the bound.
A program may use at most 128 MiB of HBM per device.

```python
import jax
import jax.numpy as jnp
from jax import lax

D = 2048
FF = 3072
TOKENS = 32768
N_TP = 4


def with_spikes(result, rng, source, target, shards_of, factor):
    owner, partner = [(jnp.arange(result.shape[dim]) // (result.shape[dim] // shards_of)).reshape([-1 if axis == dim else 1 for axis in range(result.ndim)]) for dim in (source, target)]
    chosen = jax.random.permutation(rng, shards_of)[partner]
    strong = (owner == chosen) | (owner == (partner + shards_of // 2) % shards_of)
    return jnp.where(strong, factor * result, result)


def level_of(stream_key, extent, shards, least, largest):
    factor_of, own = 1.0, jax.random.fold_in(stream_key, 6)
    for axis_at, parts in shards:
        heights = jnp.exp(jax.random.uniform(jax.random.fold_in(own, axis_at), (parts,), jnp.float32, least / len(shards), largest / len(shards)))
        factor_of = factor_of * jnp.repeat(heights, extent[axis_at] // parts).reshape([-1 if axis == axis_at else 1 for axis in range(len(extent))])
    return factor_of


def gaussian(key, extent, spread, limit, shards=(), dtype=jnp.bfloat16):
    gain = level_of(key, extent, shards, -0.22, 0.18) if shards else 1.0
    entries = jax.random.normal(key, extent, jnp.float32) * spread * gain
    return jnp.minimum(jnp.maximum(entries, -limit), limit).astype(dtype)


def gaussian_with(own_key, dims, spread, most, cuts, heavy, held_as=jnp.bfloat16):
    entries = spread * jax.random.normal(own_key, dims, jnp.float32)
    if cuts:
        entries = entries * level_of(own_key, dims, cuts, -0.22, 0.18)
    return jnp.clip(with_spikes(entries, jax.random.fold_in(own_key, 3), *heavy), -most, most).astype(held_as)


def setup_inputs(seed: int = 0) -> dict:
    streams_of = jax.random.split(jax.random.key(seed), 8)
    return {
        "x_late": gaussian(streams_of[0], (TOKENS, D), 1.0, 6.0, ((0, 256),)),
        "x_early": gaussian_with(streams_of[1], (TOKENS, D), 1.0, 24.0, ((0, 256),), (0, 1, 256, 6.0)),
        "d_hidden": gaussian_with(streams_of[2], (TOKENS, FF), 1.0, 16.0, ((0, 64), (1, 4)), (0, 1, 64, 4.0)),
        "w_gate": gaussian(streams_of[3], (D, FF), D ** -0.5, 0.125, ((0, 64), (1, 4))),
        "w_up": gaussian(streams_of[4], (D, FF), D ** -0.5, 0.125, ((0, 64), (1, 4))),
        "gate_sum": gaussian(streams_of[5], (D, FF), (0.5 * TOKENS ** 0.5), 512.0, ((0, 64), (1, 4)), jnp.float32),
        "up_sum": gaussian(streams_of[6], (D, FF), (0.5 * TOKENS ** 0.5), 512.0, ((0, 64), (1, 4)), jnp.float32),
    }


def reference(x_late, x_early, d_hidden, w_gate, w_up, gate_sum, up_sum):
    gate_late = jnp.dot(x_late, w_gate, preferred_element_type=jnp.float32)
    up_late = jnp.dot(x_late, w_up, preferred_element_type=jnp.float32)
    sigmoid_late = jax.nn.sigmoid(gate_late)
    hidden_late = (gate_late * sigmoid_late * up_late).astype(jnp.bfloat16)
    gate_early = jnp.dot(x_early, w_gate, preferred_element_type=jnp.float32)
    up_early = jnp.dot(x_early, w_up, preferred_element_type=jnp.float32)
    sigmoid_early = jax.nn.sigmoid(gate_early)
    cotangent = d_hidden.astype(jnp.float32)
    d_gate = (cotangent * up_early * sigmoid_early * (1.0 + gate_early * (1.0 - sigmoid_early))).astype(jnp.bfloat16)
    d_up = (cotangent * gate_early * sigmoid_early).astype(jnp.bfloat16)
    span = FF // N_TP
    total = jnp.zeros((x_early.shape[0], x_early.shape[1]), jnp.float32)
    for index in range(N_TP):
        lower = index * span
        partial_value = jnp.dot(d_gate[:, lower:lower + span], w_gate[:, lower:lower + span].T, preferred_element_type=jnp.float32)
        partial_value = partial_value + jnp.dot(d_up[:, lower:lower + span], w_up[:, lower:lower + span].T, preferred_element_type=jnp.float32)
        rounded = lax.optimization_barrier(partial_value.astype(jnp.bfloat16))
        total = total + rounded.astype(jnp.float32)
    grad_input = total.astype(jnp.bfloat16)
    gate_sum_out = gate_sum + jnp.dot(x_early.T, d_gate, preferred_element_type=jnp.float32)
    up_sum_out = up_sum + jnp.dot(x_early.T, d_up, preferred_element_type=jnp.float32)
    return (hidden_late, grad_input, gate_sum_out, up_sum_out)
```

```python
import jax
import jax.numpy as jnp
from jax import lax
from jax.experimental import pallas as pl
from jax.experimental.pallas import tpu as pltpu
from jax.sharding import PartitionSpec as P

Z, X, C, Y = 8, 4, 2, 4
D, HID, ROWS, SHARD = 2048, 768, 128, 32
TOK = ROWS * Y
HALF = ROWS // 2
TILE = 256
TILES = HID // TILE
MESH = pl.DeviceIdType.MESH
F32, BF16 = jnp.float32, jnp.bfloat16
MAX_COPIES = 160
LOCAL_COPIES = 12


def sigmoid(v):
    return 0.5 * jnp.tanh(0.5 * v) + 0.5


def kernel(
    x_late, x_early, d_hidden, w_gate, w_up, gate_sum, up_sum,
    hidden_out, grad_out, gate_out, up_out,
    xe, xl, wg, wu, dh, sums, xt, xtp, dg, du, pdg, pdu, su, sg,
    up_stage, up_in, up_tot, up2_stage, up2_in,
    ga_stage, ga_in, ga_tot, ga2_stage, ga2_in,
    part, y_stage, y_in, grad, hid, send_sem, recv_sem, local_sem,
):
    fs = lax.axis_index("fs")
    y = lax.axis_index("tp")
    z, x, c = fs // (X * C), (fs // C) % X, fs % C

    def at(zz, xx, cc, yy):
        return {"fs": (zz * X + xx) * C + cc, "tp": yy}

    def zk(k):
        return lax.rem(z + (k + Z), Z)

    def xk(k):
        return lax.rem(x + (k + X), X)

    def yk(k):
        return lax.rem(y + (k + Y), Y)

    zp, zm = at(zk(1), x, c, y), at(zk(-1), x, c, y)
    xp, xm = at(z, xk(1), c, y), at(z, xk(-1), c, y)
    yp, ym = at(z, x, c, yk(1)), at(z, x, c, yk(-1))
    pal = at(z, x, 1 - c, y)

    local = []

    def load(src, dst):
        copy = pltpu.make_async_copy(src, dst, local_sem.at[len(local)])
        copy.start()
        local.append(copy)
        return copy

    in_xe = [load(x_early.at[pl.ds(h * HALF, HALF)], xe.at[y, h]) for h in range(2)]
    in_wu = load(w_up, wu.at[z, x, c])
    in_wg = load(w_gate, wg.at[z, x, c])
    in_xl = [load(x_late.at[pl.ds(h * HALF, HALF)], xl.at[y, h]) for h in range(2)]
    in_dh = load(d_hidden, dh)
    in_sums = [load(gate_sum, sums.at[0]), load(up_sum, sums.at[1])]

    barrier = pltpu.get_barrier_semaphore()
    for peer in (zp, zm, xp, xm, yp, ym, pal):
        pl.semaphore_signal(barrier, inc=1, device_id=peer, device_id_type=MESH)
    pl.semaphore_wait(barrier, 7)

    copies = []

    def send(src, dst, peer):
        i = len(copies)
        copy = pltpu.make_async_remote_copy(
            src_ref=src, dst_ref=dst, send_sem=send_sem.at[i], recv_sem=recv_sem.at[i],
            device_id=peer, device_id_type=MESH,
        )
        copy.start()
        copies.append(copy)
        return copy

    def pass_on(ref, peer):
        return send(ref, ref, peer)

    for copy in (in_wu, in_wg):
        copy.wait()
    uz_p, uz_m, ux, ux_relay = {}, {}, {}, {}

    def up_x(k):
        ref = wu.at[zk(k), x, c]
        ux[k] = (pass_on(ref, xp), pass_on(ref, xm))

    def up_x_relay(k):
        for copy in ux[k]:
            copy.wait_recv()
        zz = zk(k)
        ux_relay[k] = (
            pass_on(wu.at[zz, xk(-1), c, pl.ds(0, 16)], xp),
            pass_on(wu.at[zz, xk(1), c, pl.ds(16, 16)], xm),
        )

    pal_copies = []

    def up_row(k):
        for copy in ux_relay[k]:
            copy.wait_recv()
        pal_copies.append(pass_on(wu.at[zk(k), :, c], pal))

    uz_p[0] = pass_on(wu.at[z, x, c], zp)
    uz_m[0] = pass_on(wu.at[z, x, c], zm)
    gx = (pass_on(wg.at[z, x, c], xp), pass_on(wg.at[z, x, c], xm))
    up_x(0)
    for copy in in_xe:
        copy.wait()

    def y_own(ref):
        return {
            "l0": pass_on(ref.at[y, 0], yp),
            "r1": pass_on(ref.at[y, 1], ym),
            "l1": pass_on(ref.at[y, 1], yp),
            "r0": pass_on(ref.at[y, 0], ym),
        }

    def y_relay(ref, own):
        own["l0"].wait_recv()
        own["l2"] = pass_on(ref.at[yk(-1), 0], yp)
        own["r1"].wait_recv()
        own["r2"] = pass_on(ref.at[yk(1), 1], ym)

    def turn(block):
        columns = pl.ds(pl.multiple_of(block * ROWS, ROWS), ROWS)

        def step(zz, carry):
            rows = pl.ds(pl.multiple_of(zz * TILE, TILE), TILE)
            value = xe[block, :, :, rows].reshape(ROWS, TILE)
            xt[zz, :, :, :, columns] = value.T.reshape(X, C, SHARD, ROWS)
            return carry

        lax.fori_loop(0, Z, step, 0)

    early = y_own(xe)
    turn(y)

    for copy in gx:
        copy.wait_recv()
    gx_relay = (
        pass_on(wg.at[z, xk(-1), c, pl.ds(0, 16)], xp),
        pass_on(wg.at[z, xk(1), c, pl.ds(16, 16)], xm),
    )

    def up_z(k):
        uz_p[k - 1].wait_recv()
        uz_m[k - 1].wait_recv()
        left, right = wu.at[zk(-k), x, c], wu.at[zk(k), x, c]
        if k < 3:
            uz_p[k], uz_m[k] = pass_on(left, zp), pass_on(right, zm)
        elif k == 3:
            uz_p[k] = pass_on(left.at[pl.ds(0, 16)], zp)
            uz_m[k] = pass_on(right.at[pl.ds(16, 16)], zm)
        up_x(k)
        if k < 4:
            up_x(-k)

    gz_p, gz_m = {}, {}

    def gate_block(k, sub):
        return wg.at[zk(k), pl.ds(2 * sub, 2), c]

    def gate_z(k):
        if k == 0:
            for copy in gx_relay:
                copy.wait_recv()
        for sub in range(2):
            if k and (k < 4 or sub == 0):
                gz_p[k - 1, sub].wait_recv()
            if k < 3 or (k == 3 and sub == 0):
                gz_p[k, sub] = pass_on(gate_block(-k, sub), zp)
            if k and (k < 4 or sub == 1):
                gz_m[k - 1, sub].wait_recv()
            if k < 3 or (k == 3 and sub == 1):
                gz_m[k, sub] = pass_on(gate_block(k, sub), zm)
        pal_copies.append(pass_on(wg.at[zk(k), :, c], pal))
        if 0 < k < 4:
            pal_copies.append(pass_on(wg.at[zk(-k), :, c], pal))

    up_z(1)
    gate_z(0)
    up_x_relay(0)
    up_z(2)
    y_relay(xe, early)
    for copy in in_xl:
        copy.wait()
    late = y_own(xl)
    up_x_relay(1)
    up_x_relay(-1)
    gate_z(1)
    up_z(3)
    up_row(0)
    up_x_relay(2)
    up_x_relay(-2)
    up_z(4)
    gate_z(2)
    up_row(1)
    up_row(-1)
    up_x_relay(3)
    up_x_relay(-3)
    early["l1"].wait_recv()
    early["r0"].wait_recv()
    turn(yk(-1))
    turn(yk(1))
    up_x_relay(4)
    gate_z(3)
    up_row(2)
    up_row(-2)
    early["l2"].wait_recv()
    early["r2"].wait_recv()
    turn(yk(2))
    xt_copy = send(xt.at[:, :, 1 - c], xtp, pal)
    up_row(3)
    up_row(-3)
    up_row(4)
    gate_z(4)
    in_dh.wait()
    for copy in pal_copies:
        copy.wait_recv()

    def products(rows, tile):
        span = slice(tile * TILE, (tile + 1) * TILE)
        left = rows[...].reshape(TOK, D)
        gate = jnp.dot(left, wg[..., span].reshape(D, TILE), preferred_element_type=F32)
        up = jnp.dot(left, wu[..., span].reshape(D, TILE), preferred_element_type=F32)
        return gate, up, span

    pal_d = []
    for tile in range(TILES):
        gate, up, span = products(xe, tile)
        s = sigmoid(gate)
        cot = dh[:, span].astype(F32)
        du[:, span] = (cot * gate * s).astype(BF16)
        dg[:, span] = (cot * up * s * (1.0 + gate * (1.0 - s))).astype(BF16)
        pal_d.append((send(du.at[:, span], pdu.at[:, span], pal), send(dg.at[:, span], pdg.at[:, span], pal)))

    xt_copy.wait_recv()

    def weight_grad(which, own, other, total):
        for tile in range(TILES):
            span = slice(tile * TILE, (tile + 1) * TILE)
            pal_d[tile][which].wait_recv()
            mine = xt[:, :, c].reshape(Z * X * SHARD, TOK)
            theirs = xtp[...].reshape(Z * X * SHARD, TOK)
            value = jnp.dot(mine, own[:, span], preferred_element_type=F32)
            value = value + jnp.dot(theirs, other[:, span], preferred_element_type=F32)
            total[..., span] = value.reshape(Z, X, SHARD, TILE)

    weight_grad(0, du, pdu, su)

    def up_put(i, value, peer):
        up_stage[i] = value.astype(BF16)
        return send(up_stage.at[i], up_in.at[i], peer)

    u_a1 = up_put(0, su[pl.ds(0, 4), xk(2)], xp)
    u_b1 = up_put(1, su[pl.ds(4, 4), xk(2)], xm)
    u_a2 = up_put(2, su[pl.ds(4, 4), xk(1)], xp)
    u_b2 = up_put(3, su[pl.ds(0, 4), xk(-1)], xm)
    y_relay(xl, late)

    weight_grad(1, dg, pdg, sg)

    gs_p, gs_m = {}, {}

    def ga_index(right, k, sub):
        return (k * 2 + sub) * 2 + (0 if right else 1)

    def ga_send(k, sub):
        for right, sent, peer in ((True, gs_p, zp), (False, gs_m, zm)):
            half = sub if right else 1 - sub
            value = sg[zk(k if right else -k), pl.ds(2 * half, 2)]
            if (k + 1, sub) in sent:
                sent[k + 1, sub].wait_recv()
                value = value + ga_in[ga_index(right, k + 1, sub)].astype(F32)
            i = ga_index(right, k, sub)
            ga_stage[i] = value.astype(BF16)
            sent[k, sub] = send(ga_stage.at[i], ga_in.at[i], peer)

    ga_send(4, 0)
    ga_send(3, 1)

    contract = (((1,), (1,)), ((), ()))

    def input_grad(zz, carry):
        columns = pl.ds(pl.multiple_of(zz * TILE, TILE), TILE)
        value = lax.dot_general(dg[...], wg[zz].reshape(TILE, HID), contract, preferred_element_type=F32)
        value = value + lax.dot_general(du[...], wu[zz].reshape(TILE, HID), contract, preferred_element_type=F32)
        part[:, :, :, columns] = value.astype(BF16).reshape(Y, 2, HALF, TILE)
        return carry

    lax.fori_loop(0, Z, input_grad, 0)
    y_a1 = send(part.at[yk(2), 0], y_in.at[0], yp)
    y_b1 = send(part.at[yk(2), 1], y_in.at[1], ym)
    y_a2 = send(part.at[yk(1), 1], y_in.at[2], yp)
    y_b2 = send(part.at[yk(-1), 0], y_in.at[3], ym)

    u_a1.wait_recv()
    u_a3 = up_put(4, su[pl.ds(0, 4), xk(1)] + up_in[0].astype(F32), xp)
    u_b1.wait_recv()
    u_b3 = up_put(5, su[pl.ds(4, 4), xk(-1)] + up_in[1].astype(F32), xm)
    ga_send(3, 0)
    ga_send(2, 1)
    ga_send(2, 0)

    for key in ("l1", "r0", "l2", "r2"):
        late[key].wait_recv()

    hid_copies = []

    def late_tile(tile):
        gate, up, span = products(xl, tile)
        hid[:, span] = (gate * sigmoid(gate) * up).astype(BF16)
        hid_copies.append(load(hid.at[:, span], hidden_out.at[:, span]))

    late_tile(0)
    ga_send(1, 1)
    ga_send(1, 0)

    for copy in (u_a2, u_b2, u_a3, u_b3):
        copy.wait_recv()
    up_tot[pl.ds(0, 4)] = su[pl.ds(0, 4), x] + up_in[4].astype(F32) + up_in[3].astype(F32)
    up_tot[pl.ds(4, 4)] = su[pl.ds(4, 4), x] + up_in[2].astype(F32) + up_in[5].astype(F32)

    u2_p, u2_m = {}, {}

    def up2(k):
        for right, sent, peer in ((True, u2_p, zp), (False, u2_m, zm)):
            i = 2 * (k - 1) + (0 if right else 1)
            j = i + 2
            dest = zk(k if right else -k)
            h = 0 if right else 1
            near, far = pl.ds(16 * h, 16), pl.ds(16 * (1 - h), 16)
            if k == 4:
                up2_stage[i, near] = up_tot[dest, near].astype(BF16)
                sent[k] = send(up2_stage.at[i, near], up2_in.at[i, near], peer)
                continue
            sent[k + 1].wait_recv()
            if k == 3:
                up2_stage[i, near] = (up_tot[dest, near] + up2_in[j, near].astype(F32)).astype(BF16)
                up2_stage[i, far] = up_tot[dest, far].astype(BF16)
            else:
                up2_stage[i] = (up_tot[dest] + up2_in[j].astype(F32)).astype(BF16)
            sent[k] = send(up2_stage.at[i], up2_in.at[i], peer)

    up2(4)
    late_tile(1)
    up2(3)

    y_a1.wait_recv()
    y_stage[0] = (part[yk(1), 0].astype(F32) + y_in[0].astype(F32)).astype(BF16)
    y_a3 = send(y_stage.at[0], y_in.at[4], yp)
    y_b1.wait_recv()
    y_stage[1] = (part[yk(-1), 1].astype(F32) + y_in[1].astype(F32)).astype(BF16)
    y_b3 = send(y_stage.at[1], y_in.at[5], ym)

    up2(2)
    late_tile(2)
    up2(1)

    for sent in (gs_p, gs_m):
        sent[1, 0].wait_recv()
        sent[1, 1].wait_recv()
    for half in range(2):
        rows = pl.ds(2 * half, 2)
        ga_tot[rows] = (
            sg[z, rows]
            + ga_in[ga_index(True, 1, half)].astype(F32)
            + ga_in[ga_index(False, 1, 1 - half)].astype(F32)
        )

    lo, hi = pl.ds(0, 16), pl.ds(16, 16)
    ga2_stage[0, lo] = ga_tot[xk(2), lo].astype(BF16)
    g_a1 = send(ga2_stage.at[0, lo], ga2_in.at[0, lo], xp)
    ga2_stage[1, hi] = ga_tot[xk(2), hi].astype(BF16)
    g_b1 = send(ga2_stage.at[1, hi], ga2_in.at[1, hi], xm)
    g_a1.wait_recv()
    ga2_stage[2, lo] = (ga_tot[xk(1), lo] + ga2_in[0, lo].astype(F32)).astype(BF16)
    ga2_stage[2, hi] = ga_tot[xk(1), hi].astype(BF16)
    g_a3 = send(ga2_stage.at[2], ga2_in.at[2], xp)
    g_b1.wait_recv()
    ga2_stage[3, hi] = (ga_tot[xk(-1), hi] + ga2_in[1, hi].astype(F32)).astype(BF16)
    ga2_stage[3, lo] = ga_tot[xk(-1), lo].astype(BF16)
    g_b3 = send(ga2_stage.at[3], ga2_in.at[3], xm)

    for copy in in_sums:
        copy.wait()
    u2_p[1].wait_recv()
    u2_m[1].wait_recv()
    sums[1] = sums[1] + (up_tot[z] + up2_in[0].astype(F32) + up2_in[1].astype(F32))
    out_up = load(sums.at[1], up_out)

    g_a3.wait_recv()
    g_b3.wait_recv()
    sums[0] = sums[0] + (ga_tot[x] + ga2_in[2].astype(F32) + ga2_in[3].astype(F32))
    out_gate = load(sums.at[0], gate_out)

    for copy in (y_a2, y_b2, y_a3, y_b3):
        copy.wait_recv()
    grad[pl.ds(0, HALF)] = (part[y, 0].astype(F32) + y_in[4].astype(F32) + y_in[3].astype(F32)).astype(BF16)
    grad[pl.ds(HALF, HALF)] = (part[y, 1].astype(F32) + y_in[2].astype(F32) + y_in[5].astype(F32)).astype(BF16)
    out_grad = load(grad, grad_out)

    for copy in copies:
        copy.wait_send()
    for copy in (*hid_copies, out_up, out_gate, out_grad):
        copy.wait()


def local(*args):
    any_space = pl.BlockSpec(memory_space=pl.ANY)
    vmem = pltpu.VMEM
    flops = 4 * 2 * TOK * D * HID * 2
    return tuple(
        pl.pallas_call(
            kernel,
            out_shape=(
                jax.ShapeDtypeStruct((TOK, HID), BF16),
                jax.ShapeDtypeStruct((ROWS, D), BF16),
                jax.ShapeDtypeStruct((SHARD, HID), F32),
                jax.ShapeDtypeStruct((SHARD, HID), F32),
            ),
            in_specs=[any_space] * 7,
            out_specs=[any_space] * 4,
            scratch_shapes=[
                vmem((Y, 2, HALF, D), BF16),
                vmem((Y, 2, HALF, D), BF16),
                vmem((Z, X, C, SHARD, HID), BF16),
                vmem((Z, X, C, SHARD, HID), BF16),
                vmem((TOK, HID), BF16),
                vmem((2, SHARD, HID), F32),
                vmem((Z, X, C, SHARD, TOK), BF16),
                vmem((Z, X, SHARD, TOK), BF16),
                vmem((TOK, HID), BF16),
                vmem((TOK, HID), BF16),
                vmem((TOK, HID), BF16),
                vmem((TOK, HID), BF16),
                vmem((Z, X, SHARD, HID), F32),
                vmem((Z, X, SHARD, HID), F32),
                vmem((6, 4, SHARD, HID), BF16),
                vmem((6, 4, SHARD, HID), BF16),
                vmem((Z, SHARD, HID), F32),
                vmem((8, SHARD, HID), BF16),
                vmem((8, SHARD, HID), BF16),
                vmem((20, 2, SHARD, HID), BF16),
                vmem((20, 2, SHARD, HID), BF16),
                vmem((X, SHARD, HID), F32),
                vmem((4, SHARD, HID), BF16),
                vmem((4, SHARD, HID), BF16),
                vmem((Y, 2, HALF, D), BF16),
                vmem((2, HALF, D), BF16),
                vmem((6, HALF, D), BF16),
                vmem((ROWS, D), BF16),
                vmem((TOK, HID), BF16),
                pltpu.SemaphoreType.DMA((MAX_COPIES,)),
                pltpu.SemaphoreType.DMA((MAX_COPIES,)),
                pltpu.SemaphoreType.DMA((24,)),
            ],
            compiler_params=pltpu.CompilerParams(
                collective_id=0, has_side_effects=True, vmem_limit_bytes=63 * 1024 * 1024
            ),
            cost_estimate=pl.CostEstimate(flops=flops, bytes_accessed=8 << 20, transcendentals=0),
            name="layer",
        )(*args)
    )


def solution(mesh):
    return jax.shard_map(
        local,
        mesh=mesh,
        in_specs=(
            P(("fs", "tp"), None),
            P(("fs", "tp"), None),
            P("fs", "tp"),
            P("fs", "tp"),
            P("fs", "tp"),
            P("fs", "tp"),
            P("fs", "tp"),
        ),
        out_specs=(P("fs", "tp"), P(("fs", "tp"), None), P("fs", "tp"), P("fs", "tp")),
        check_vma=False,
    )
```

```python
import jax
import jax.numpy as jnp
from jax import lax
from jax.experimental import pallas as pl
from jax.experimental.pallas import tpu as pltpu
from jax.sharding import PartitionSpec as P

Z, X, C, Y = 8, 4, 2, 4
D, HID, ROWS, SHARD = 2048, 768, 128, 32
BOTH = 2 * HID
NA = 640
NB = BOTH - NA
TOK = ROWS * Y
HALF = ROWS // 2
TILE = 256
MESH = pl.DeviceIdType.MESH
F32, BF16 = jnp.float32, jnp.bfloat16
DIRS = (1, -1)
COPIES, SENDS = 202, 100
ORDER = (
    ("own",), ("t", 0), ("ax1",), ("bz", 1), ("az", 0, 1), ("bx", 0), ("ax2",), ("ar", 0), ("az", 1, 1),
    ("az", -1, 1), ("xer",), ("xlo",), ("bx", 1), ("bz", 2), ("br", 0), ("az", 0, 2), ("az", 2, 1), ("ar", 1),
    ("az", 1, 2), ("br", 1), ("az", -1, 2), ("bz", 3), ("t", 1), ("az", 0, 3), ("bx", 2), ("f", 0), ("f", 1),
    ("az", 2, 2), ("ar", 2), ("az", 1, 3), ("az", -1, 3), ("bz", 4), ("az", 0, 4), ("bx", 3), ("br", 2),
    ("t", 2), ("az", 2, 3), ("ar", 3), ("az", 1, 4), ("az", -1, 4), ("bx", 4), ("f", 2), ("br", 3),
    ("az", 2, 4), ("ar", 4), ("br", 4), ("f", 3), ("f", 4), ("f2",), ("e", 1), ("e", 0), ("xlr",), ("e", 2),
    ("i", 3), ("i", 1), ("i", 0), ("w", 4), ("w", 3), ("y1", 0), ("i", 2), ("y1", 1), ("sz", 2, 3), ("sx", 4),
    ("sz", 1, 3), ("w", 2), ("sz", -1, 3), ("l", 1), ("sz", 2, 2), ("sx", 3), ("st", 4), ("sz", 0, 3),
    ("y2", 0), ("w", 1), ("sz", 1, 2), ("sx", 2), ("sz", -1, 2), ("w", 0), ("sz", 2, 1), ("l", 0), ("st", 3),
    ("sb", 3), ("sz", 0, 2), ("l", 2), ("sx", 1), ("sz", -1, 1), ("y2", 1), ("sz", 1, 1), ("at", 2),
    ("st", 2), ("sb", 2), ("sx", 0), ("sz", 0, 1), ("at", -1), ("at", 1), ("yf", 0), ("st", 1), ("sa",),
    ("sb", 1), ("at", 0), ("st", 0), ("yf", 1), ("fa",), ("fb",),
)


def sigmoid(v):
    return 0.5 * jnp.tanh(0.5 * v) + 0.5


def rows_of(k):
    return (k,) if k in (0, 4) else (k, -k)


def kernel(
    x_late, x_early, d_hidden, w_gate, w_up, gate_sum, up_sum,
    hidden_out, grad_out, gate_out, up_out,
    xe, xl, w, dh, sums, xt, xtp, d, pd, acc, s, ta, tb,
    a_stage, a_in, b_stage, b_in, part, y_stage, y_in,
    send_sem, recv_sem, local_sem,
):
    fs = lax.axis_index("fs")
    y = lax.axis_index("tp")
    z, x, c = fs // (X * C), (fs // C) % X, fs % C

    def zk(k):
        return lax.rem(z + (k + Z), Z)

    def xk(k):
        return lax.rem(x + (k + X), X)

    def yk(k):
        return lax.rem(y + (k + Y), Y)

    def at(zz, xx, cc, yy):
        return {"fs": (zz * X + xx) * C + cc, "tp": yy}

    zp = {k: at(zk(k), x, c, y) for k in DIRS}
    xp = {k: at(z, xk(k), c, y) for k in DIRS}
    yp = {k: at(z, x, c, yk(k)) for k in DIRS}
    pal = at(z, x, 1 - c, y)

    local = []

    def load(src, dst):
        copy = pltpu.make_async_copy(src, dst, local_sem.at[len(local)])
        copy.start()
        local.append(copy)
        return copy

    in_w = [
        load(w_up, w.at[z, x, c, :, pl.ds(HID, HID)]),
        load(w_gate, w.at[z, x, c, :, pl.ds(0, HID)]),
    ]
    in_xe = [load(x_early.at[pl.ds(h * HALF, HALF)], xe.at[y, h]) for h in range(2)]
    in_xl = [load(x_late.at[pl.ds(h * HALF, HALF)], xl.at[y, h]) for h in range(2)]
    in_dh = load(d_hidden, dh)
    in_sums = [load(gate_sum, sums.at[:, pl.ds(0, HID)]), load(up_sum, sums.at[:, pl.ds(HID, HID)])]

    with jax.named_scope("entry"):
        barrier = pltpu.get_barrier_semaphore()
        for peer in (*zp.values(), *xp.values(), *yp.values(), pal):
            pl.semaphore_signal(barrier, inc=1, device_id=peer, device_id_type=MESH)
        pl.semaphore_wait(barrier, 7)

    msgs, order = {}, []

    def send(key, src, dst, peer):
        i = len(msgs)
        if i >= SENDS:
            order[i - SENDS].wait_send()
        copy = pltpu.make_async_remote_copy(
            src_ref=src, dst_ref=dst, send_sem=send_sem.at[i % SENDS], recv_sem=recv_sem.at[i],
            device_id=peer, device_id_type=MESH,
        )
        order.append(copy)
        copy.start()
        msgs[key] = copy

    def push(key, ref, peer):
        send(key, ref, ref, peer)

    def wait(*key):
        msgs[key].wait_recv()

    def half(k):
        return pl.ds(0, 16) if k > 0 else pl.ds(16, 16)

    ALL = pl.ds(0, SHARD)
    CA, CB = pl.ds(0, NA), pl.ds(NA, NB)

    def own():
        for copy in in_w:
            copy.wait()
        for k in DIRS:
            push(("bz", 0, k), w.at[z, x, c, :, CB], zp[k])
        for k in DIRS:
            push(("ax", k), w.at[z, x, c, :, CA], xp[k])
        for k in DIRS:
            push(("bx", 0, k), w.at[z, x, c, :, CB], xp[k])
        for k in DIRS:
            push(("az", 0, 0, k), w.at[z, x, c, :, CA], zp[k])
        for copy in in_xe:
            copy.wait()
        y_own("xe", xe)

    def y_own(name, ref):
        for i in range(2):
            for k in DIRS:
                h = i if k > 0 else 1 - i
                push((name, i, k), ref.at[y, h], yp[k])

    def y_relay(name, ref):
        for k in DIRS:
            wait(name, 0, k)
            push((name, 2, k), ref.at[yk(-k), 0 if k > 0 else 1], yp[k])

    def xl_own():
        for copy in in_xl:
            copy.wait()
        y_own("xl", xl)

    def turn(block):
        tokens = pl.ds(pl.multiple_of(block * ROWS, ROWS), ROWS)

        def step(zz, carry):
            span = pl.ds(pl.multiple_of(zz * TILE, TILE), TILE)
            value = xe[block, :, :, span].reshape(ROWS, TILE)
            xt[zz, :, :, :, tokens] = value.T.reshape(X, C, SHARD, ROWS)
            return carry

        lax.fori_loop(0, Z, step, 0)
        return tokens

    def turns(which):
        if which == 1:
            for k in DIRS:
                wait("xe", 1, k)
        if which == 2:
            for k in DIRS:
                wait("xe", 2, k)
        for k in (1, -1) if which == 1 else (which,):
            tokens = turn(yk(k))
            send(("xt", k), xt.at[:, :, 1 - c, :, tokens], xtp.at[:, :, :, tokens], pal)

    def ax1():
        for k in DIRS:
            wait("ax", k)
        for k in DIRS:
            push(("axr", k), w.at[z, xk(-k), c, half(k), CA], xp[k])
        for j in DIRS:
            for k in DIRS:
                push(("az", j, 0, k), w.at[z, xk(j), c, :, CA], zp[k])

    def ax2():
        for k in DIRS:
            wait("axr", k)
        for k in DIRS:
            push(("az", 2, 0, k), w.at[z, xk(2), c, :, CA], zp[k])

    def az(j, n):
        for k in DIRS:
            wait("az", j, n - 1, k)
        if n < 4:
            for k in DIRS:
                rows = half(k) if n == 3 else ALL
                push(("az", j, n, k), w.at[zk(-k * n), xk(j), c, rows, CA], zp[k])

    def ar(n):
        for r in rows_of(n):
            push(("ar", r), w.at[zk(r), :, c, :, CA], pal)

    def bz(n):
        for k in DIRS:
            wait("bz", n - 1, k)
        if n < 4:
            for k in DIRS:
                rows = half(k) if n == 3 else ALL
                push(("bz", n, k), w.at[zk(-k * n), x, c, rows, CB], zp[k])
        for r in rows_of(n):
            for k in DIRS:
                push(("bx", r, k), w.at[zk(r), x, c, :, CB], xp[k])

    def bx(n):
        for r in rows_of(n):
            for k in DIRS:
                wait("bx", r, k)
                push(("bxr", r, k), w.at[zk(r), xk(-k), c, half(k), CB], xp[k])

    def br(n):
        for r in rows_of(n):
            for k in DIRS:
                wait("bxr", r, k)
            push(("br", r), w.at[zk(r), :, c, :, CB], pal)

    def dot(a, b):
        return jnp.dot(a, b, preferred_element_type=F32)

    near = (0, 1, -1)

    def f(n):
        left, right = [], []
        for r in rows_of(n):
            wait("ar", r)
            wait("br", r)
            span = pl.ds(pl.multiple_of(zk(r) * TILE, TILE), TILE)
            left.append(jnp.concatenate([xe[yk(k), :, :, span].reshape(ROWS, TILE) for k in near], axis=0))
            right.append(w[zk(r)].reshape(TILE, BOTH))
        value = dot(jnp.concatenate(left, axis=1), jnp.concatenate(right, axis=0))
        for i, k in enumerate(near):
            piece = value[i * ROWS : (i + 1) * ROWS]
            acc[yk(k)] = piece if n == 0 else acc[yk(k)] + piece

    def f2():
        for copy in (in_dh, *in_sums):
            copy.wait()
        left = xe[yk(2)].reshape(ROWS, D)
        for t in range(BOTH // TILE):
            span = pl.ds(t * TILE, TILE)
            acc[yk(2), :, span] = dot(left, w[..., span].reshape(D, TILE))

    def e(t):
        lo, hi = pl.ds(t * TILE, TILE), pl.ds(HID + t * TILE, TILE)
        gate = acc[..., lo].reshape(TOK, TILE)
        up = acc[..., hi].reshape(TOK, TILE)
        sig = sigmoid(gate)
        cot = dh[:, lo].astype(F32) * sig
        d[:, lo] = (cot * up * (1.0 + gate * (1.0 - sig))).astype(BF16)
        d[:, hi] = (cot * gate).astype(BF16)
        send(("d", t, 0), d.at[:, lo], pd.at[:, lo], pal)
        send(("d", t, 1), d.at[:, hi], pd.at[:, hi], pal)

    lates = []

    def late(t):
        if not lates:
            for i in (1, 2):
                for k in DIRS:
                    wait("xl", i, k)
        lates.append(t)
        lo, hi = pl.ds(t * TILE, TILE), pl.ds(HID + t * TILE, TILE)
        left = xl[...].reshape(TOK, D)
        gate = dot(left, w[..., lo].reshape(D, TILE))
        up = dot(left, w[..., hi].reshape(D, TILE))
        hidden_out[:, lo] = (gate * sigmoid(gate) * up).astype(BF16)

    slots = {}

    def slot(kind, key):
        return slots.setdefault((kind, key), sum(1 for name in slots if name[0] == kind))

    def sent(kind, key, value, peer, rows=ALL, more=None, more_rows=None):
        stage, into = (a_stage, a_in) if kind == "a" else (b_stage, b_in)
        i = slot(kind, key)
        stage[i, rows] = value.astype(BF16)
        if more is not None:
            stage[i, more_rows] = more.astype(BF16)
            rows = ALL
        send(key, stage.at[i, rows], into.at[i, rows], peer)

    def came(kind, *key):
        wait(*key)
        ref = a_in if kind == "a" else b_in
        return ref, slot(kind, key)

    def wgrad(n):
        if n == 4:
            for t in range(3):
                wait("d", t, 0)
                wait("d", t, 1)
            for k in (0, 1, -1, 2):
                wait("xt", k)
        rows = rows_of(n)
        mine = jnp.concatenate([xt[zk(r), :, c].reshape(X * SHARD, TOK) for r in rows], axis=0)
        theirs = jnp.concatenate([xtp[zk(r)].reshape(X * SHARD, TOK) for r in rows], axis=0)
        value = dot(mine, d[...]) + dot(theirs, pd[...])
        for i, r in enumerate(rows):
            s[zk(r)] = value[i * X * SHARD : (i + 1) * X * SHARD].reshape(X, SHARD, BOTH)
        for r in rows:
            for k in DIRS:
                sent("b", ("sx", r, 2, k), s[zk(r), xk(2), half(k), CB], xp[k], half(k))
        if n == 4:
            for j in (2, 1, -1, 0):
                for k in DIRS:
                    sent("a", ("sz", j, 4, k), s[zk(4), xk(j), half(k), CA], zp[k], half(k))

    def onward(kind, before, key, own, peer, partly, k):
        ref, i = came(kind, *before)
        if partly:
            mine, rest = half(k), half(-k)
            sent(kind, key, own(mine) + ref[i, mine].astype(F32), peer, mine, own(rest), rest)
        else:
            sent(kind, key, own(ALL) + ref[i].astype(F32), peer)

    def sx(n):
        for r in rows_of(n):
            for k in DIRS:
                onward("b", ("sx", r, 2, k), ("sx", r, 1, k), lambda q: s[zk(r), xk(k), q, CB], xp[k], True, k)

    def both(kind, own, *key):
        value = own
        for k in DIRS:
            ref, i = came(kind, *key, k)
            value = value + ref[i].astype(F32)
        return value

    def st(n):
        for r in rows_of(n):
            tb[zk(r)] = both("b", s[zk(r), x, :, CB], "sx", r, 1)
        if n == 4:
            for k in DIRS:
                sent("b", ("sb", 4, k), tb[zk(4), half(k)], zp[k], half(k))

    def sb(n):
        for k in DIRS:
            onward("b", ("sb", n + 1, k), ("sb", n, k), lambda q: tb[zk(k * n), q], zp[k], n == 3, k)

    def fb():
        value = sums[:, CB] + both("b", tb[z], "sb", 1)
        gate_out[:, pl.ds(NA, HID - NA)] = value[:, : HID - NA]
        up_out[...] = value[:, HID - NA :]

    def sz(j, n):
        for k in DIRS:
            onward("a", ("sz", j, n + 1, k), ("sz", j, n, k), lambda q: s[zk(k * n), xk(j), q, CA], zp[k], n == 3, k)

    def at_x(j):
        ta[xk(j)] = both("a", s[z, xk(j), :, CA], "sz", j, 1)
        if j == 2:
            for k in DIRS:
                sent("a", ("sa", 2, k), ta[xk(2), half(k)], xp[k], half(k))

    def sa():
        for k in DIRS:
            onward("a", ("sa", 2, k), ("sa", 1, k), lambda q: ta[xk(k), q], xp[k], True, k)

    def fa():
        gate_out[:, CA] = sums[:, CA] + both("a", ta[x], "sa", 1)

    def igrad(n):
        span = pl.ds(n * 2 * TILE, 2 * TILE)
        weights = w[2 * n : 2 * n + 2].reshape(2 * TILE, BOTH)
        value = lax.dot_general(d[...], weights, (((1,), (1,)), ((), ())), preferred_element_type=F32)
        part[..., span] = value.astype(BF16).reshape(Y, 2, HALF, 2 * TILE)

    def y_cols(h):
        return pl.ds(h * (D // 2), D // 2)

    def y1(h):
        for m, which in ((2, 2), (3, 1)):
            for k in DIRS:
                side = (0 if k > 0 else 1) if m == 2 else (1 if k > 0 else 0)
                i = 4 * h + 2 * (m - 2) + (0 if k > 0 else 1)
                send(("y", h, m, k), part.at[yk(which * k), side, :, y_cols(h)], y_in.at[i], yp[k])

    def y2(h):
        for k in DIRS:
            i = 0 if k > 0 else 1
            wait("y", h, 2, k)
            value = part[yk(k), i, :, y_cols(h)].astype(F32) + y_in[4 * h + i].astype(F32)
            y_stage[2 * h + i] = value.astype(BF16)
            send(("y", h, 1, k), y_stage.at[2 * h + i], y_in.at[8 + 2 * h + i], yp[k])

    def yf(h):
        for k in DIRS:
            wait("y", h, 1, k)
            wait("y", h, 3, k)
        for side in range(2):
            value = part[y, side, :, y_cols(h)].astype(F32)
            value = value + y_in[8 + 2 * h + side].astype(F32)
            value = value + y_in[4 * h + 2 + (1 - side)].astype(F32)
            grad_out[pl.ds(side * HALF, HALF), y_cols(h)] = value.astype(BF16)

    tasks = {
        "own": own, "t": turns, "xer": lambda: y_relay("xe", xe), "xlo": xl_own,
        "xlr": lambda: y_relay("xl", xl), "ax1": ax1, "ax2": ax2, "az": az, "ar": ar, "bz": bz, "bx": bx,
        "br": br, "f": f, "f2": f2, "e": e, "w": wgrad, "sx": sx, "st": st, "sb": sb, "fb": fb, "sz": sz,
        "at": at_x, "sa": sa, "fa": fa, "i": igrad, "y1": y1, "y2": y2, "yf": yf, "l": late,
    }
    for name, *args in ORDER:
        with jax.named_scope("_".join(map(str, (name, *args)))):
            tasks[name](*args)
    with jax.named_scope("drain"):
        for copy in order[-SENDS:]:
            copy.wait_send()


def local(*args):
    hbm_space = pl.BlockSpec(memory_space=pltpu.HBM)
    vmem_space = pl.BlockSpec(memory_space=pltpu.VMEM)
    vmem = pltpu.VMEM
    return tuple(
        pl.pallas_call(
            kernel,
            out_shape=OUTS,
            in_specs=[hbm_space] * 7,
            out_specs=[vmem_space] * 4,
            scratch_shapes=[
                vmem((Y, 2, HALF, D), BF16),
                vmem((Y, 2, HALF, D), BF16),
                vmem((Z, X, C, SHARD, BOTH), BF16),
                vmem((TOK, HID), BF16),
                vmem((SHARD, BOTH), F32),
                vmem((Z, X, C, SHARD, TOK), BF16),
                vmem((Z, X, SHARD, TOK), BF16),
                vmem((TOK, BOTH), BF16),
                vmem((TOK, BOTH), BF16),
                vmem((Y, ROWS, BOTH), F32),
                vmem((Z, X, SHARD, BOTH), F32),
                vmem((X, SHARD, NA), F32),
                vmem((Z, SHARD, NB), F32),
                vmem((36, SHARD, NA), BF16),
                vmem((36, SHARD, NA), BF16),
                vmem((40, SHARD, NB), BF16),
                vmem((40, SHARD, NB), BF16),
                vmem((Y, 2, HALF, D), BF16),
                vmem((4, HALF, D // 2), BF16),
                vmem((12, HALF, D // 2), BF16),
                pltpu.SemaphoreType.DMA((SENDS,)),
                pltpu.SemaphoreType.DMA((COPIES,)),
                pltpu.SemaphoreType.DMA((16,)),
            ],
            compiler_params=pltpu.CompilerParams(
                collective_id=0, has_side_effects=True, vmem_limit_bytes=VMEM_MIB * 1024 * 1024
            ),
            cost_estimate=pl.CostEstimate(flops=8 * TOK * D * BOTH, bytes_accessed=8 << 20, transcendentals=0),
            name="layer",
        )(*args)
    )


OUTS = (
    jax.ShapeDtypeStruct((TOK, HID), BF16),
    jax.ShapeDtypeStruct((ROWS, D), BF16),
    jax.ShapeDtypeStruct((SHARD, HID), F32),
    jax.ShapeDtypeStruct((SHARD, HID), F32),
)
VMEM_MIB = 60


def solution(mesh):
    return jax.shard_map(
        local,
        mesh=mesh,
        in_specs=(
            P(("fs", "tp"), None),
            P(("fs", "tp"), None),
            P("fs", "tp"),
            P("fs", "tp"),
            P("fs", "tp"),
            P("fs", "tp"),
            P("fs", "tp"),
        ),
        out_specs=(P("fs", "tp"), P(("fs", "tp"), None), P("fs", "tp"), P("fs", "tp")),
        check_vma=False,
    )
```

```python
import jax
import jax.numpy as jnp
from jax import lax
from jax.experimental import pallas as pl
from jax.experimental.pallas import tpu as pltpu
from jax.sharding import PartitionSpec as P

Z, X, C, Y = 8, 4, 2, 4
D, HID, ROWS, SHARD = 2048, 768, 128, 32
BOTH = 2 * HID
NA = 640
NB = BOTH - NA
TOK = ROWS * Y
HALF = ROWS // 2
TILE = 256
MESH = pl.DeviceIdType.MESH
F32, BF16 = jnp.float32, jnp.bfloat16
DIRS = (1, -1)
GROUPS, SIZED = 96, 11264
ORDER = (
    ("own",), ("t", 0), ("ax1",), ("bz", 1), ("az", 0, 1), ("bx", 0), ("ax2",), ("ar", 0), ("az", 1, 1),
    ("az", -1, 1), ("xer",), ("xlo",), ("bx", 1), ("bz", 2), ("br", 0), ("az", 0, 2), ("az", 2, 1), ("ar", 1),
    ("az", 1, 2), ("br", 1), ("az", -1, 2), ("bz", 3), ("t", 1), ("az", 0, 3), ("bx", 2), ("f", 0), ("f", 1),
    ("az", 2, 2), ("ar", 2), ("az", 1, 3), ("az", -1, 3), ("bz", 4), ("az", 0, 4), ("bx", 3), ("br", 2),
    ("t", 2), ("az", 2, 3), ("ar", 3), ("az", 1, 4), ("az", -1, 4), ("bx", 4), ("f", 2), ("br", 3),
    ("az", 2, 4), ("ar", 4), ("br", 4), ("f", 3), ("f", 4), ("f2",), ("e", 1), ("e", 0), ("xlr",), ("e", 2),
    ("i", 3), ("i", 1), ("i", 0), ("w", 4), ("w", 3), ("y1", 0), ("i", 2), ("y1", 1), ("sz", 2, 3), ("sx", 4),
    ("sz", 1, 3), ("w", 2), ("sz", -1, 3), ("l", 1), ("sz", 2, 2), ("sx", 3), ("st", 4), ("sz", 0, 3),
    ("y2", 0), ("w", 1), ("sz", 1, 2), ("sx", 2), ("sz", -1, 2), ("w", 0), ("sz", 2, 1), ("l", 0), ("st", 3),
    ("sb", 3), ("sz", 0, 2), ("l", 2), ("sx", 1), ("sz", -1, 1), ("y2", 1), ("sz", 1, 1), ("at", 2),
    ("st", 2), ("sb", 2), ("sx", 0), ("sz", 0, 1), ("at", -1), ("at", 1), ("yf", 0), ("st", 1), ("sa",),
    ("sb", 1), ("at", 0), ("st", 0), ("yf", 1), ("fa",), ("fb",),
)


def sigmoid(v):
    return 0.5 * jnp.tanh(0.5 * v) + 0.5


def rows_of(k):
    return (k,) if k in (0, 4) else (k, -k)


def group_of(key):
    name = key[0]
    if name in ("xt", "d"):
        return (name,)
    if name == "xe":
        return (name, key[1])
    if name == "xl":
        return (name, min(key[1], 1))
    if name in ("ar", "br"):
        return ("row", abs(key[1]))
    if name in ("bx", "bxr"):
        return (name, abs(key[1]))
    if name == "sx":
        return (name, abs(key[1]), key[2])
    if name == "y":
        return (name, key[1], 2 if key[2] == 2 else 1)
    return key[:-1]


def kernel(
    x_late, x_early, d_hidden, w_gate, w_up, gate_sum, up_sum,
    hidden_out, grad_out, gate_out, up_out,
    xe, xl, w, dh, sums, xt, xtp, d, pd, acc, s, ta, tb,
    a_stage, a_in, b_stage, b_in, part, y_stage, y_in, hid, grad, sized,
    send_sem, recv_sem, local_sem,
):
    fs = lax.axis_index("fs")
    y = lax.axis_index("tp")
    z, x, c = fs // (X * C), (fs // C) % X, fs % C

    def zk(k):
        return lax.rem(z + (k + Z), Z)

    def xk(k):
        return lax.rem(x + (k + X), X)

    def yk(k):
        return lax.rem(y + (k + Y), Y)

    def at(zz, xx, cc, yy):
        return {"fs": (zz * X + xx) * C + cc, "tp": yy}

    zp = {k: at(zk(k), x, c, y) for k in DIRS}
    xp = {k: at(z, xk(k), c, y) for k in DIRS}
    yp = {k: at(z, x, c, yk(k)) for k in DIRS}
    pal = at(z, x, 1 - c, y)

    local = []

    def load(src, dst):
        copy = pltpu.make_async_copy(src, dst, local_sem.at[len(local)])
        copy.start()
        local.append(copy)
        return copy

    stores = []

    def store(src, dst):
        stores.append(load(src, dst))

    in_w = [
        load(w_up, w.at[z, x, c, :, pl.ds(HID, HID)]),
        load(w_gate, w.at[z, x, c, :, pl.ds(0, HID)]),
    ]
    in_xe = [load(x_early.at[pl.ds(h * HALF, HALF)], xe.at[y, h]) for h in range(2)]
    in_xl = [load(x_late.at[pl.ds(h * HALF, HALF)], xl.at[y, h]) for h in range(2)]
    in_dh = load(d_hidden, dh)
    in_sums = [load(gate_sum, sums.at[:, pl.ds(0, HID)]), load(up_sum, sums.at[:, pl.ds(HID, HID)])]

    with jax.named_scope("entry"):
        barrier = pltpu.get_barrier_semaphore()
        for peer in (*zp.values(), *xp.values(), *yp.values(), pal):
            pl.semaphore_signal(barrier, inc=1, device_id=peer, device_id_type=MESH)
        pl.semaphore_wait(barrier, 7)

    groups, links = {}, {}

    def taken(sem, size):
        ref = sized.at[pl.ds(0, size // 512)]
        pltpu.make_async_copy(ref, ref, sem).wait()

    def send(key, src, dst, peer):
        group, link = group_of(key), id(peer)
        into = groups.setdefault(group, [len(groups), 0, False])
        out = links.setdefault(link, [len(links), 0])
        if into[2]:
            raise ValueError(key)
        pltpu.make_async_remote_copy(
            src_ref=src, dst_ref=dst, send_sem=send_sem.at[out[0]], recv_sem=recv_sem.at[into[0]],
            device_id=peer, device_id_type=MESH,
        ).start()
        size = src.dtype.itemsize
        for extent in src.shape:
            size *= extent
        into[1] += size
        out[1] += size

    def push(key, ref, peer):
        send(key, ref, ref, peer)

    def wait(*group):
        into = groups[group]
        if not into[2]:
            into[2] = True
            taken(recv_sem.at[into[0]], into[1])

    def half(k):
        return pl.ds(0, 16) if k > 0 else pl.ds(16, 16)

    ALL = pl.ds(0, SHARD)
    CA, CB = pl.ds(0, NA), pl.ds(NA, NB)

    def own():
        for copy in in_w:
            copy.wait()
        for k in DIRS:
            push(("bz", 0, k), w.at[z, x, c, :, CB], zp[k])
        for k in DIRS:
            push(("ax", k), w.at[z, x, c, :, CA], xp[k])
        for k in DIRS:
            push(("bx", 0, k), w.at[z, x, c, :, CB], xp[k])
        for k in DIRS:
            push(("az", 0, 0, k), w.at[z, x, c, :, CA], zp[k])
        for copy in in_xe:
            copy.wait()
        y_own("xe", xe)

    def y_own(name, ref):
        for i in range(2):
            for k in DIRS:
                h = i if k > 0 else 1 - i
                push((name, i, k), ref.at[y, h], yp[k])

    def y_relay(name, ref):
        wait(name, 0)
        for k in DIRS:
            push((name, 2, k), ref.at[yk(-k), 0 if k > 0 else 1], yp[k])

    def xl_own():
        for copy in in_xl:
            copy.wait()
        y_own("xl", xl)

    def turn(block):
        tokens = pl.ds(pl.multiple_of(block * ROWS, ROWS), ROWS)

        def step(zz, carry):
            span = pl.ds(pl.multiple_of(zz * TILE, TILE), TILE)
            value = xe[block, :, :, span].reshape(ROWS, TILE)
            xt[zz, :, :, :, tokens] = value.T.reshape(X, C, SHARD, ROWS)
            return carry

        lax.fori_loop(0, Z, step, 0)
        return tokens

    def turns(which):
        if which == 1:
            wait("xe", 1)
        if which == 2:
            wait("xe", 2)
        for k in (1, -1) if which == 1 else (which,):
            tokens = turn(yk(k))
            send(("xt", k), xt.at[:, :, 1 - c, :, tokens], xtp.at[:, :, :, tokens], pal)

    def ax1():
        wait("ax")
        for k in DIRS:
            push(("axr", k), w.at[z, xk(-k), c, half(k), CA], xp[k])
        for j in DIRS:
            for k in DIRS:
                push(("az", j, 0, k), w.at[z, xk(j), c, :, CA], zp[k])

    def ax2():
        wait("axr")
        for k in DIRS:
            push(("az", 2, 0, k), w.at[z, xk(2), c, :, CA], zp[k])

    def az(j, n):
        wait("az", j, n - 1)
        if n < 4:
            for k in DIRS:
                rows = half(k) if n == 3 else ALL
                push(("az", j, n, k), w.at[zk(-k * n), xk(j), c, rows, CA], zp[k])

    def ar(n):
        for r in rows_of(n):
            push(("ar", r), w.at[zk(r), :, c, :, CA], pal)

    def bz(n):
        wait("bz", n - 1)
        if n < 4:
            for k in DIRS:
                rows = half(k) if n == 3 else ALL
                push(("bz", n, k), w.at[zk(-k * n), x, c, rows, CB], zp[k])
        for r in rows_of(n):
            for k in DIRS:
                push(("bx", r, k), w.at[zk(r), x, c, :, CB], xp[k])

    def bx(n):
        wait("bx", n)
        for r in rows_of(n):
            for k in DIRS:
                push(("bxr", r, k), w.at[zk(r), xk(-k), c, half(k), CB], xp[k])

    def br(n):
        wait("bxr", n)
        for r in rows_of(n):
            push(("br", r), w.at[zk(r), :, c, :, CB], pal)

    def dot(a, b):
        return jnp.dot(a, b, preferred_element_type=F32)

    near = (0, 1, -1)

    def f(n):
        left, right = [], []
        wait("row", n)
        for r in rows_of(n):
            span = pl.ds(pl.multiple_of(zk(r) * TILE, TILE), TILE)
            left.append(jnp.concatenate([xe[yk(k), :, :, span].reshape(ROWS, TILE) for k in near], axis=0))
            right.append(w[zk(r)].reshape(TILE, BOTH))
        value = dot(jnp.concatenate(left, axis=1), jnp.concatenate(right, axis=0))
        for i, k in enumerate(near):
            piece = value[i * ROWS : (i + 1) * ROWS]
            acc[yk(k)] = piece if n == 0 else acc[yk(k)] + piece

    def f2():
        for copy in (in_dh, *in_sums):
            copy.wait()
        left = xe[yk(2)].reshape(ROWS, D)
        for t in range(BOTH // TILE):
            span = pl.ds(t * TILE, TILE)
            acc[yk(2), :, span] = dot(left, w[..., span].reshape(D, TILE))

    def e(t):
        lo, hi = pl.ds(t * TILE, TILE), pl.ds(HID + t * TILE, TILE)
        gate = acc[..., lo].reshape(TOK, TILE)
        up = acc[..., hi].reshape(TOK, TILE)
        sig = sigmoid(gate)
        cot = dh[:, lo].astype(F32) * sig
        d[:, lo] = (cot * up * (1.0 + gate * (1.0 - sig))).astype(BF16)
        d[:, hi] = (cot * gate).astype(BF16)
        send(("d", t, 0), d.at[:, lo], pd.at[:, lo], pal)
        send(("d", t, 1), d.at[:, hi], pd.at[:, hi], pal)

    lates = []

    def late(t):
        if not lates:
            wait("xl", 1)
        lates.append(t)
        lo, hi = pl.ds(t * TILE, TILE), pl.ds(HID + t * TILE, TILE)
        left = xl[...].reshape(TOK, D)
        gate = dot(left, w[..., lo].reshape(D, TILE))
        up = dot(left, w[..., hi].reshape(D, TILE))
        hid[:, lo] = (gate * sigmoid(gate) * up).astype(BF16)
        store(hid.at[:, lo], hidden_out.at[:, lo])

    slots = {}

    def slot(kind, key):
        return slots.setdefault((kind, key), sum(1 for name in slots if name[0] == kind))

    def sent(kind, key, value, peer, rows=ALL, more=None, more_rows=None):
        stage, into = (a_stage, a_in) if kind == "a" else (b_stage, b_in)
        i = slot(kind, key)
        stage[i, rows] = value.astype(BF16)
        if more is not None:
            stage[i, more_rows] = more.astype(BF16)
            rows = ALL
        send(key, stage.at[i, rows], into.at[i, rows], peer)

    def came(kind, *key):
        wait(*group_of(key))
        ref = a_in if kind == "a" else b_in
        return ref, slot(kind, key)

    def wgrad(n):
        if n == 4:
            wait("d")
            wait("xt")
        rows = rows_of(n)
        mine = jnp.concatenate([xt[zk(r), :, c].reshape(X * SHARD, TOK) for r in rows], axis=0)
        theirs = jnp.concatenate([xtp[zk(r)].reshape(X * SHARD, TOK) for r in rows], axis=0)
        value = dot(mine, d[...]) + dot(theirs, pd[...])
        for i, r in enumerate(rows):
            s[zk(r)] = value[i * X * SHARD : (i + 1) * X * SHARD].reshape(X, SHARD, BOTH)
        for r in rows:
            for k in DIRS:
                sent("b", ("sx", r, 2, k), s[zk(r), xk(2), half(k), CB], xp[k], half(k))
        if n == 4:
            for j in (2, 1, -1, 0):
                for k in DIRS:
                    sent("a", ("sz", j, 4, k), s[zk(4), xk(j), half(k), CA], zp[k], half(k))

    def onward(kind, before, key, own, peer, partly, k):
        ref, i = came(kind, *before)
        if partly:
            mine, rest = half(k), half(-k)
            sent(kind, key, own(mine) + ref[i, mine].astype(F32), peer, mine, own(rest), rest)
        else:
            sent(kind, key, own(ALL) + ref[i].astype(F32), peer)

    def sx(n):
        for r in rows_of(n):
            for k in DIRS:
                onward("b", ("sx", r, 2, k), ("sx", r, 1, k), lambda q: s[zk(r), xk(k), q, CB], xp[k], True, k)

    def both(kind, own, *key):
        value = own
        for k in DIRS:
            ref, i = came(kind, *key, k)
            value = value + ref[i].astype(F32)
        return value

    def st(n):
        for r in rows_of(n):
            tb[zk(r)] = both("b", s[zk(r), x, :, CB], "sx", r, 1)
        if n == 4:
            for k in DIRS:
                sent("b", ("sb", 4, k), tb[zk(4), half(k)], zp[k], half(k))

    def sb(n):
        for k in DIRS:
            onward("b", ("sb", n + 1, k), ("sb", n, k), lambda q: tb[zk(k * n), q], zp[k], n == 3, k)

    def fb():
        sums[:, CB] = sums[:, CB] + both("b", tb[z], "sb", 1)
        store(sums.at[:, pl.ds(NA, HID - NA)], gate_out.at[:, pl.ds(NA, HID - NA)])
        store(sums.at[:, pl.ds(HID, HID)], up_out)

    def sz(j, n):
        for k in DIRS:
            onward("a", ("sz", j, n + 1, k), ("sz", j, n, k), lambda q: s[zk(k * n), xk(j), q, CA], zp[k], n == 3, k)

    def at_x(j):
        ta[xk(j)] = both("a", s[z, xk(j), :, CA], "sz", j, 1)
        if j == 2:
            for k in DIRS:
                sent("a", ("sa", 2, k), ta[xk(2), half(k)], xp[k], half(k))

    def sa():
        for k in DIRS:
            onward("a", ("sa", 2, k), ("sa", 1, k), lambda q: ta[xk(k), q], xp[k], True, k)

    def fa():
        sums[:, CA] = sums[:, CA] + both("a", ta[x], "sa", 1)
        store(sums.at[:, CA], gate_out.at[:, CA])

    def igrad(n):
        span = pl.ds(n * 2 * TILE, 2 * TILE)
        weights = w[2 * n : 2 * n + 2].reshape(2 * TILE, BOTH)
        value = lax.dot_general(d[...], weights, (((1,), (1,)), ((), ())), preferred_element_type=F32)
        part[..., span] = value.astype(BF16).reshape(Y, 2, HALF, 2 * TILE)

    def y_cols(h):
        return pl.ds(h * (D // 2), D // 2)

    def y1(h):
        for m, which in ((2, 2), (3, 1)):
            for k in DIRS:
                side = (0 if k > 0 else 1) if m == 2 else (1 if k > 0 else 0)
                i = 4 * h + 2 * (m - 2) + (0 if k > 0 else 1)
                send(("y", h, m, k), part.at[yk(which * k), side, :, y_cols(h)], y_in.at[i], yp[k])

    def y2(h):
        for k in DIRS:
            i = 0 if k > 0 else 1
            wait("y", h, 2)
            value = part[yk(k), i, :, y_cols(h)].astype(F32) + y_in[4 * h + i].astype(F32)
            y_stage[2 * h + i] = value.astype(BF16)
            send(("y", h, 1, k), y_stage.at[2 * h + i], y_in.at[8 + 2 * h + i], yp[k])

    def yf(h):
        wait("y", h, 1)
        for side in range(2):
            value = part[y, side, :, y_cols(h)].astype(F32)
            value = value + y_in[8 + 2 * h + side].astype(F32)
            value = value + y_in[4 * h + 2 + (1 - side)].astype(F32)
            grad[pl.ds(side * HALF, HALF), y_cols(h)] = value.astype(BF16)
        store(grad.at[:, y_cols(h)], grad_out.at[:, y_cols(h)])

    tasks = {
        "own": own, "t": turns, "xer": lambda: y_relay("xe", xe), "xlo": xl_own,
        "xlr": lambda: y_relay("xl", xl), "ax1": ax1, "ax2": ax2, "az": az, "ar": ar, "bz": bz, "bx": bx,
        "br": br, "f": f, "f2": f2, "e": e, "w": wgrad, "sx": sx, "st": st, "sb": sb, "fb": fb, "sz": sz,
        "at": at_x, "sa": sa, "fa": fa, "i": igrad, "y1": y1, "y2": y2, "yf": yf, "l": late,
    }
    for name, *args in ORDER:
        with jax.named_scope("_".join(map(str, (name, *args)))):
            tasks[name](*args)
    with jax.named_scope("drain"):
        for i, size in links.values():
            taken(send_sem.at[i], size)
        for copy in stores:
            copy.wait()


def finish(*refs):
    ins, outs, held, sems = refs[:4], refs[4:8], refs[8:12], refs[12]
    into = [pltpu.make_async_copy(a, b, sems.at[0, i]) for i, (a, b) in enumerate(zip(ins, held))]
    out = [pltpu.make_async_copy(a, b, sems.at[1, i]) for i, (a, b) in enumerate(zip(held, outs))]
    for copy in into:
        copy.start()
    for first, second in zip(into, out):
        first.wait()
        second.start()
    for copy in out:
        copy.wait()


def local(*args):
    any_space = pl.BlockSpec(memory_space=pl.ANY)
    vmem = pltpu.VMEM
    held = pl.pallas_call(
            kernel,
            out_shape=OUTS,
            in_specs=[any_space] * 7,
            out_specs=[any_space] * 4,
            scratch_shapes=[
                vmem((Y, 2, HALF, D), BF16),
                vmem((Y, 2, HALF, D), BF16),
                vmem((Z, X, C, SHARD, BOTH), BF16),
                vmem((TOK, HID), BF16),
                vmem((SHARD, BOTH), F32),
                vmem((Z, X, C, SHARD, TOK), BF16),
                vmem((Z, X, SHARD, TOK), BF16),
                vmem((TOK, BOTH), BF16),
                vmem((TOK, BOTH), BF16),
                vmem((Y, ROWS, BOTH), F32),
                vmem((Z, X, SHARD, BOTH), F32),
                vmem((X, SHARD, NA), F32),
                vmem((Z, SHARD, NB), F32),
                vmem((36, SHARD, NA), BF16),
                vmem((36, SHARD, NA), BF16),
                vmem((40, SHARD, NB), BF16),
                vmem((40, SHARD, NB), BF16),
                vmem((Y, 2, HALF, D), BF16),
                vmem((4, HALF, D // 2), BF16),
                vmem((12, HALF, D // 2), BF16),
                vmem((TOK, HID), BF16),
                vmem((ROWS, D), BF16),
                vmem((SIZED, 128), F32),
                pltpu.SemaphoreType.DMA((7,)),
                pltpu.SemaphoreType.DMA((GROUPS,)),
                pltpu.SemaphoreType.DMA((20,)),
            ],
            compiler_params=pltpu.CompilerParams(
                collective_id=0, has_side_effects=True, vmem_limit_bytes=VMEM_MIB * 1024 * 1024
            ),
            cost_estimate=pl.CostEstimate(flops=8 * TOK * D * BOTH, bytes_accessed=8 << 20, transcendentals=0),
            name="layer",
        )(*args)
    return tuple(
        pl.pallas_call(
            finish,
            out_shape=OUTS,
            in_specs=[any_space] * 4,
            out_specs=[any_space] * 4,
            scratch_shapes=[*(vmem(a.shape, a.dtype) for a in OUTS), pltpu.SemaphoreType.DMA((2, 4))],
            name="finish",
        )(*held)
    )


OUTS = (
    jax.ShapeDtypeStruct((TOK, HID), BF16),
    jax.ShapeDtypeStruct((ROWS, D), BF16),
    jax.ShapeDtypeStruct((SHARD, HID), F32),
    jax.ShapeDtypeStruct((SHARD, HID), F32),
)
VMEM_MIB = 60


def solution(mesh):
    return jax.shard_map(
        local,
        mesh=mesh,
        in_specs=(
            P(("fs", "tp"), None),
            P(("fs", "tp"), None),
            P("fs", "tp"),
            P("fs", "tp"),
            P("fs", "tp"),
            P("fs", "tp"),
            P("fs", "tp"),
        ),
        out_specs=(P("fs", "tp"), P(("fs", "tp"), None), P("fs", "tp"), P("fs", "tp")),
        check_vma=False,
    )
```

```python
import jax
import jax.numpy as jnp
from jax import lax
from jax.experimental import pallas as pl
from jax.experimental.pallas import tpu as pltpu
from jax.sharding import PartitionSpec as P

Z, X, C, Y = 8, 4, 2, 4
D, HID, ROWS, SHARD = 2048, 768, 128, 32
BOTH = 2 * HID
NA = 640
NB = BOTH - NA
TOK = ROWS * Y
HALF = ROWS // 2
TILE = 256
MESH = pl.DeviceIdType.MESH
F32, BF16 = jnp.float32, jnp.bfloat16
DIRS = (1, -1)
GROUPS, SIZED = 96, 11264
ORDER = (
    ("own",), ("ax1",), ("bz", 1), ("az0",), ("bx", 0), ("bzx", 1), ("ax2",), ("bz", 2), ("az", 0, 1),
    ("bzx", 2), ("az", -1, 1), ("t", 0), ("az", 1, 1), ("xer",), ("ar", 0), ("bx", 1), ("bz", 3),
    ("az", 2, 1), ("xlo",), ("br", 0), ("bzx", 3), ("bx", 2), ("ar", 1), ("az", 0, 2), ("az", -1, 2),
    ("az", 1, 2), ("bzx", 4), ("br", 1), ("az", 2, 2), ("t", 1), ("ar", 2), ("bx", 3), ("az", 0, 3),
    ("az", -1, 3), ("f", 0), ("az", 1, 3), ("br", 2), ("f", 1), ("az", 2, 3), ("bx", 4), ("ar", 3), ("t", 2),
    ("az", -1, 4), ("br", 3), ("f", 2), ("f2",), ("az", 1, 4), ("az", 0, 4), ("az", 2, 4), ("ar", 4),
    ("br", 4), ("f", 3), ("f", 4), ("e", -1), ("xlr",), ("e", 2), ("e", 0), ("e", 1), ("i", 3), ("i", 2),
    ("i", 0), ("w", 4), ("w", 3), ("w", 2), ("sz", 2, 3), ("sx", 4), ("y1", 1), ("sz", 1, 3), ("i", 1),
    ("sz", -1, 3), ("y1", 0), ("sz", 0, 3), ("sx", 3), ("sz", 2, 2), ("w", 1), ("st", 4), ("w", 0),
    ("sz", 1, 2), ("sz", -1, 2), ("sx", 2), ("sz", 2, 1), ("st", 3), ("sb", 3), ("sz", 0, 2), ("y2", 1),
    ("bz", 4), ("sx", 1), ("sz", 1, 1), ("l", 2), ("sz", -1, 1), ("y2", 0), ("st", 2), ("at", 2), ("sb", 2),
    ("l", 1), ("sx", 0), ("l", 0), ("at", 1), ("st", 1), ("sz", 0, 1), ("sb", 1), ("at", -1), ("sa",),
    ("at", 0), ("yf", 1), ("st", 0), ("fa",), ("fb",), ("yf", 0),
)


def sigmoid(v):
    return 0.5 * jnp.tanh(0.5 * v) + 0.5


def rows_of(k):
    return (k,) if k in (0, 4) else (k, -k)


def group_of(key):
    name = key[0]
    if name in ("xt", "d"):
        return (name,)
    if name == "xe":
        return (name, key[1])
    if name == "xl":
        return (name, min(key[1], 1))
    if name in ("ar", "br"):
        return ("row", abs(key[1]))
    if name in ("bx", "bxr"):
        return (name, abs(key[1]))
    if name == "sx":
        return (name, abs(key[1]), key[2])
    if name == "y":
        return (name, key[1], 2 if key[2] == 2 else 1)
    return key[:-1]


def kernel(
    x_late, x_early, d_hidden, w_gate, w_up, gate_sum, up_sum,
    hidden_out, grad_out, gate_out, up_out,
    xe, xl, w, dh, sums, xt, xtp, d, pd, acc, s, ta, tb,
    a_stage, a_in, b_stage, b_in, part, y_stage, y_in, hid, grad, sized,
    send_sem, recv_sem, local_sem,
):
    fs = lax.axis_index("fs")
    y = lax.axis_index("tp")
    z, x, c = fs // (X * C), (fs // C) % X, fs % C

    def zk(k):
        return lax.rem(z + (k + Z), Z)

    def xk(k):
        return lax.rem(x + (k + X), X)

    def yk(k):
        return lax.rem(y + (k + Y), Y)

    def at(zz, xx, cc, yy):
        return {"fs": (zz * X + xx) * C + cc, "tp": yy}

    zp = {k: at(zk(k), x, c, y) for k in DIRS}
    xp = {k: at(z, xk(k), c, y) for k in DIRS}
    yp = {k: at(z, x, c, yk(k)) for k in DIRS}
    pal = at(z, x, 1 - c, y)

    local = []

    def load(src, dst):
        copy = pltpu.make_async_copy(src, dst, local_sem.at[len(local)])
        copy.start()
        local.append(copy)
        return copy

    stores = []

    def store(src, dst):
        stores.append(load(src, dst))

    in_w = [
        load(w_up, w.at[z, x, c, :, pl.ds(HID, HID)]),
        load(w_gate, w.at[z, x, c, :, pl.ds(0, HID)]),
    ]
    in_xe = [load(x_early.at[pl.ds(h * HALF, HALF)], xe.at[y, h]) for h in range(2)]
    in_xl = [load(x_late.at[pl.ds(h * HALF, HALF)], xl.at[y, h]) for h in range(2)]
    in_dh = [load(d_hidden.at[pl.ds(i * ROWS, ROWS)], dh.at[i]) for i in range(Y)]
    in_sums = [load(gate_sum, sums.at[:, pl.ds(0, HID)]), load(up_sum, sums.at[:, pl.ds(HID, HID)])]

    with jax.named_scope("entry"):
        barrier = pltpu.get_barrier_semaphore()
        for peer in (*zp.values(), *xp.values(), *yp.values(), pal):
            pl.semaphore_signal(barrier, inc=1, device_id=peer, device_id_type=MESH)
        pl.semaphore_wait(barrier, 7)

    groups, links = {}, {}

    def taken(sem, size):
        ref = sized.at[pl.ds(0, size // 512)]
        pltpu.make_async_copy(ref, ref, sem).wait()

    def send(key, src, dst, peer):
        group, link = group_of(key), id(peer)
        into = groups.setdefault(group, [len(groups), 0, False])
        out = links.setdefault(link, [len(links), 0])
        if into[2]:
            raise ValueError(key)
        pltpu.make_async_remote_copy(
            src_ref=src, dst_ref=dst, send_sem=send_sem.at[out[0]], recv_sem=recv_sem.at[into[0]],
            device_id=peer, device_id_type=MESH,
        ).start()
        size = src.dtype.itemsize
        for extent in src.shape:
            size *= extent
        into[1] += size
        out[1] += size

    def push(key, ref, peer):
        send(key, ref, ref, peer)

    def wait(*group):
        into = groups[group]
        if not into[2]:
            into[2] = True
            taken(recv_sem.at[into[0]], into[1])

    def half(k):
        return pl.ds(0, 16) if k > 0 else pl.ds(16, 16)

    ALL = pl.ds(0, SHARD)
    CA, CB = pl.ds(0, NA), pl.ds(NA, NB)

    def own():
        for copy in in_w:
            copy.wait()
        for k in DIRS:
            push(("bz", 0, k), w.at[z, x, c, :, CB], zp[k])
        for k in DIRS:
            push(("ax", k), w.at[z, x, c, :, CA], xp[k])
        for k in DIRS:
            push(("bx", 0, k), w.at[z, x, c, :, CB], xp[k])
        for k in DIRS:
            push(("az", 0, 0, k), w.at[z, x, c, :, CA], zp[k])
        for copy in in_xe:
            copy.wait()
        y_own("xe", xe)

    def y_own(name, ref):
        for i in range(2):
            for k in DIRS:
                h = i if k > 0 else 1 - i
                push((name, i, k), ref.at[y, h], yp[k])

    def y_relay(name, ref):
        wait(name, 0)
        for k in DIRS:
            push((name, 2, k), ref.at[yk(-k), 0 if k > 0 else 1], yp[k])

    def xl_own():
        for copy in in_xl:
            copy.wait()
        y_own("xl", xl)

    def turn(block):
        tokens = pl.ds(pl.multiple_of(block * ROWS, ROWS), ROWS)

        def step(zz, carry):
            span = pl.ds(pl.multiple_of(zz * TILE, TILE), TILE)
            value = xe[block, :, :, span].reshape(ROWS, TILE)
            xt[zz, :, :, :, tokens] = value.T.reshape(X, C, SHARD, ROWS)
            return carry

        lax.fori_loop(0, Z, step, 0)
        return tokens

    def turns(which):
        if which == 1:
            wait("xe", 1)
        if which == 2:
            wait("xe", 2)
        for k in (1, -1) if which == 1 else (which,):
            tokens = turn(yk(k))
            send(("xt", k), xt.at[:, :, 1 - c, :, tokens], xtp.at[:, :, :, tokens], pal)

    def ax1():
        wait("ax")
        for k in DIRS:
            push(("axr", k), w.at[z, xk(-k), c, half(k), CA], xp[k])

    def az0():
        wait("ax")
        for j in DIRS:
            for k in DIRS:
                push(("az", j, 0, k), w.at[z, xk(j), c, :, CA], zp[k])

    def ax2():
        wait("axr")
        for k in DIRS:
            push(("az", 2, 0, k), w.at[z, xk(2), c, :, CA], zp[k])

    def az(j, n):
        wait("az", j, n - 1)
        if n < 4:
            for k in DIRS:
                rows = half(k) if n == 3 else ALL
                push(("az", j, n, k), w.at[zk(-k * n), xk(j), c, rows, CA], zp[k])

    def ar(n):
        for r in rows_of(n):
            push(("ar", r), w.at[zk(r), :, c, :, CA], pal)

    def bz(n):
        wait("bz", n - 1)
        if n < 4:
            for k in DIRS:
                rows = half(k) if n == 3 else ALL
                push(("bz", n, k), w.at[zk(-k * n), x, c, rows, CB], zp[k])

    def bzx(n):
        wait("bz", n - 1)
        for r in rows_of(n):
            for k in DIRS:
                push(("bx", r, k), w.at[zk(r), x, c, :, CB], xp[k])

    def bx(n):
        wait("bx", n)
        for r in rows_of(n):
            for k in DIRS:
                push(("bxr", r, k), w.at[zk(r), xk(-k), c, half(k), CB], xp[k])

    def br(n):
        wait("bxr", n)
        for r in rows_of(n):
            push(("br", r), w.at[zk(r), :, c, :, CB], pal)

    def dot(a, b):
        return jnp.dot(a, b, preferred_element_type=F32)

    def rows_product(rows, blocks):
        spans = [pl.ds(pl.multiple_of(zk(r) * TILE, TILE), TILE) for r in rows]
        left = [[xe[yk(b), :, :, q].reshape(ROWS, TILE) for q in spans] for b in blocks]
        left = jnp.concatenate([jnp.concatenate(q, axis=1) for q in left], axis=0)
        right = jnp.concatenate([w[zk(r)].reshape(TILE, BOTH) for r in rows], axis=0)
        value = dot(left, right)
        return [(yk(b), value[i * ROWS : (i + 1) * ROWS]) for i, b in enumerate(blocks)]

    def f(n):
        wait("row", n)
        for block, piece in rows_product(rows_of(n), (0, 1, -1) if n < 3 else (0, 1, -1, 2)):
            acc[block] = piece if n == 0 else acc[block] + piece

    def f2():
        for copy in (*in_dh, *in_sums):
            copy.wait()
        for block, piece in rows_product((0, 1, -1, 2, -2), (2,)):
            acc[block] = piece

    def e(b):
        block = yk(b)
        gate, up = acc[block, :, :HID], acc[block, :, HID:]
        sig = sigmoid(gate)
        cot = dh[block].astype(F32) * sig
        d[block, :, :HID] = (cot * up * (1.0 + gate * (1.0 - sig))).astype(BF16)
        d[block, :, HID:] = (cot * gate).astype(BF16)
        send(("d", b), d.at[block], pd.at[block], pal)

    lates = []

    def late(t):
        if not lates:
            wait("xl", 1)
        lates.append(t)
        lo, hi = pl.ds(t * TILE, TILE), pl.ds(HID + t * TILE, TILE)
        left = xl[...].reshape(TOK, D)
        gate = dot(left, w[..., lo].reshape(D, TILE))
        up = dot(left, w[..., hi].reshape(D, TILE))
        hid[:, lo] = (gate * sigmoid(gate) * up).astype(BF16)
        store(hid.at[:, lo], hidden_out.at[:, lo])

    slots = {}

    def slot(kind, key):
        return slots.setdefault((kind, key), sum(1 for name in slots if name[0] == kind))

    def sent(kind, key, value, peer, rows=ALL, more=None, more_rows=None):
        stage, into = (a_stage, a_in) if kind == "a" else (b_stage, b_in)
        i = slot(kind, key)
        stage[i, rows] = value.astype(BF16)
        if more is not None:
            stage[i, more_rows] = more.astype(BF16)
            rows = ALL
        send(key, stage.at[i, rows], into.at[i, rows], peer)

    def came(kind, *key):
        wait(*group_of(key))
        ref = a_in if kind == "a" else b_in
        return ref, slot(kind, key)

    def wgrad(n):
        if n == 4:
            wait("d")
            wait("xt")
        rows = rows_of(n)
        mine = jnp.concatenate([xt[zk(r), :, c].reshape(X * SHARD, TOK) for r in rows], axis=0)
        theirs = jnp.concatenate([xtp[zk(r)].reshape(X * SHARD, TOK) for r in rows], axis=0)
        value = dot(mine, d[...].reshape(TOK, BOTH)) + dot(theirs, pd[...].reshape(TOK, BOTH))
        for i, r in enumerate(rows):
            s[zk(r)] = value[i * X * SHARD : (i + 1) * X * SHARD].reshape(X, SHARD, BOTH)
        for r in rows:
            for k in DIRS:
                sent("b", ("sx", r, 2, k), s[zk(r), xk(2), half(k), CB], xp[k], half(k))
        if n == 4:
            for j in (2, 1, -1, 0):
                for k in DIRS:
                    sent("a", ("sz", j, 4, k), s[zk(4), xk(j), half(k), CA], zp[k], half(k))

    def onward(kind, before, key, own, peer, partly, k):
        ref, i = came(kind, *before)
        if partly:
            mine, rest = half(k), half(-k)
            sent(kind, key, own(mine) + ref[i, mine].astype(F32), peer, mine, own(rest), rest)
        else:
            sent(kind, key, own(ALL) + ref[i].astype(F32), peer)

    def sx(n):
        for r in rows_of(n):
            for k in DIRS:
                onward("b", ("sx", r, 2, k), ("sx", r, 1, k), lambda q: s[zk(r), xk(k), q, CB], xp[k], True, k)

    def both(kind, own, *key):
        value = own
        for k in DIRS:
            ref, i = came(kind, *key, k)
            value = value + ref[i].astype(F32)
        return value

    def st(n):
        for r in rows_of(n):
            tb[zk(r)] = both("b", s[zk(r), x, :, CB], "sx", r, 1)
        if n == 4:
            for k in DIRS:
                sent("b", ("sb", 4, k), tb[zk(4), half(k)], zp[k], half(k))

    def sb(n):
        for k in DIRS:
            onward("b", ("sb", n + 1, k), ("sb", n, k), lambda q: tb[zk(k * n), q], zp[k], n == 3, k)

    def fb():
        sums[:, CB] = sums[:, CB] + both("b", tb[z], "sb", 1)
        store(sums.at[:, pl.ds(NA, HID - NA)], gate_out.at[:, pl.ds(NA, HID - NA)])
        store(sums.at[:, pl.ds(HID, HID)], up_out)

    def sz(j, n):
        for k in DIRS:
            onward("a", ("sz", j, n + 1, k), ("sz", j, n, k), lambda q: s[zk(k * n), xk(j), q, CA], zp[k], n == 3, k)

    def at_x(j):
        ta[xk(j)] = both("a", s[z, xk(j), :, CA], "sz", j, 1)
        if j == 2:
            for k in DIRS:
                sent("a", ("sa", 2, k), ta[xk(2), half(k)], xp[k], half(k))

    def sa():
        for k in DIRS:
            onward("a", ("sa", 2, k), ("sa", 1, k), lambda q: ta[xk(k), q], xp[k], True, k)

    def fa():
        sums[:, CA] = sums[:, CA] + both("a", ta[x], "sa", 1)
        store(sums.at[:, CA], gate_out.at[:, CA])

    def igrad(n):
        span = pl.ds(n * 2 * TILE, 2 * TILE)
        weights = w[2 * n : 2 * n + 2].reshape(2 * TILE, BOTH)
        value = lax.dot_general(d[...].reshape(TOK, BOTH), weights, (((1,), (1,)), ((), ())), preferred_element_type=F32)
        part[..., span] = value.astype(BF16).reshape(Y, 2, HALF, 2 * TILE)

    def y_cols(h):
        return pl.ds(h * (D // 2), D // 2)

    def y1(h):
        for m, which in ((2, 2), (3, 1)):
            for k in DIRS:
                side = (0 if k > 0 else 1) if m == 2 else (1 if k > 0 else 0)
                i = 4 * h + 2 * (m - 2) + (0 if k > 0 else 1)
                send(("y", h, m, k), part.at[yk(which * k), side, :, y_cols(h)], y_in.at[i], yp[k])

    def y2(h):
        for k in DIRS:
            i = 0 if k > 0 else 1
            wait("y", h, 2)
            value = part[yk(k), i, :, y_cols(h)].astype(F32) + y_in[4 * h + i].astype(F32)
            y_stage[2 * h + i] = value.astype(BF16)
            send(("y", h, 1, k), y_stage.at[2 * h + i], y_in.at[8 + 2 * h + i], yp[k])

    def yf(h):
        wait("y", h, 1)
        for side in range(2):
            value = part[y, side, :, y_cols(h)].astype(F32)
            value = value + y_in[8 + 2 * h + side].astype(F32)
            value = value + y_in[4 * h + 2 + (1 - side)].astype(F32)
            grad[pl.ds(side * HALF, HALF), y_cols(h)] = value.astype(BF16)
        store(grad.at[:, y_cols(h)], grad_out.at[:, y_cols(h)])

    tasks = {
        "own": own, "t": turns, "xer": lambda: y_relay("xe", xe), "xlo": xl_own,
        "xlr": lambda: y_relay("xl", xl), "ax1": ax1, "az0": az0, "bzx": bzx, "ax2": ax2, "az": az, "ar": ar, "bz": bz, "bx": bx,
        "br": br, "f": f, "f2": f2, "e": e, "w": wgrad, "sx": sx, "st": st, "sb": sb, "fb": fb, "sz": sz,
        "at": at_x, "sa": sa, "fa": fa, "i": igrad, "y1": y1, "y2": y2, "yf": yf, "l": late,
    }
    for name, *args in ORDER:
        with jax.named_scope("_".join(map(str, (name, *args)))):
            tasks[name](*args)
    with jax.named_scope("drain"):
        for i, size in links.values():
            taken(send_sem.at[i], size)
        for copy in stores:
            copy.wait()


def finish(*refs):
    ins, outs, held, sems = refs[:4], refs[4:8], refs[8:12], refs[12]
    into = [pltpu.make_async_copy(a, b, sems.at[0, i]) for i, (a, b) in enumerate(zip(ins, held))]
    out = [pltpu.make_async_copy(a, b, sems.at[1, i]) for i, (a, b) in enumerate(zip(held, outs))]
    for copy in into:
        copy.start()
    for first, second in zip(into, out):
        first.wait()
        second.start()
    for copy in out:
        copy.wait()


def local(*args):
    any_space = pl.BlockSpec(memory_space=pl.ANY)
    vmem = pltpu.VMEM
    held = pl.pallas_call(
            kernel,
            out_shape=OUTS,
            in_specs=[any_space] * 7,
            out_specs=[any_space] * 4,
            scratch_shapes=[
                vmem((Y, 2, HALF, D), BF16),
                vmem((Y, 2, HALF, D), BF16),
                vmem((Z, X, C, SHARD, BOTH), BF16),
                vmem((Y, ROWS, HID), BF16),
                vmem((SHARD, BOTH), F32),
                vmem((Z, X, C, SHARD, TOK), BF16),
                vmem((Z, X, SHARD, TOK), BF16),
                vmem((Y, ROWS, BOTH), BF16),
                vmem((Y, ROWS, BOTH), BF16),
                vmem((Y, ROWS, BOTH), F32),
                vmem((Z, X, SHARD, BOTH), F32),
                vmem((X, SHARD, NA), F32),
                vmem((Z, SHARD, NB), F32),
                vmem((36, SHARD, NA), BF16),
                vmem((36, SHARD, NA), BF16),
                vmem((40, SHARD, NB), BF16),
                vmem((40, SHARD, NB), BF16),
                vmem((Y, 2, HALF, D), BF16),
                vmem((4, HALF, D // 2), BF16),
                vmem((12, HALF, D // 2), BF16),
                vmem((TOK, HID), BF16),
                vmem((ROWS, D), BF16),
                vmem((SIZED, 128), F32),
                pltpu.SemaphoreType.DMA((7,)),
                pltpu.SemaphoreType.DMA((GROUPS,)),
                pltpu.SemaphoreType.DMA((20,)),
            ],
            compiler_params=pltpu.CompilerParams(
                collective_id=0, has_side_effects=True, vmem_limit_bytes=VMEM_MIB * 1024 * 1024
            ),
            cost_estimate=pl.CostEstimate(flops=8 * TOK * D * BOTH, bytes_accessed=8 << 20, transcendentals=0),
            name="layer",
        )(*args)
    return tuple(
        pl.pallas_call(
            finish,
            out_shape=OUTS,
            in_specs=[any_space] * 4,
            out_specs=[any_space] * 4,
            scratch_shapes=[*(vmem(a.shape, a.dtype) for a in OUTS), pltpu.SemaphoreType.DMA((2, 4))],
            name="finish",
        )(*held)
    )


OUTS = (
    jax.ShapeDtypeStruct((TOK, HID), BF16),
    jax.ShapeDtypeStruct((ROWS, D), BF16),
    jax.ShapeDtypeStruct((SHARD, HID), F32),
    jax.ShapeDtypeStruct((SHARD, HID), F32),
)
VMEM_MIB = 60


def solution(mesh):
    return jax.shard_map(
        local,
        mesh=mesh,
        in_specs=(
            P(("fs", "tp"), None),
            P(("fs", "tp"), None),
            P("fs", "tp"),
            P("fs", "tp"),
            P("fs", "tp"),
            P("fs", "tp"),
            P("fs", "tp"),
        ),
        out_specs=(P("fs", "tp"), P(("fs", "tp"), None), P("fs", "tp"), P("fs", "tp")),
        check_vma=False,
    )
```

```python
import jax
import jax.numpy as jnp
from jax import lax
from jax.experimental import pallas as pl
from jax.experimental.pallas import tpu as pltpu
from jax.sharding import PartitionSpec as P

Z, X, C, Y = 8, 4, 2, 4
D, HID, ROWS, SHARD = 2048, 768, 128, 32
BOTH = 2 * HID
NA = 640
NB = BOTH - NA
TOK = ROWS * Y
HALF = ROWS // 2
TILE = 256
MESH = pl.DeviceIdType.MESH
F32, BF16 = jnp.float32, jnp.bfloat16
DIRS = (1, -1)
GROUPS, SIZED = 79, 11264
ORDER = (
    ("own",), ("bz", 1, 1), ("ax1",), ("bz", 1, -1), ("bx", 0), ("bzx", 1), ("az0",), ("t", 0), ("az", 0, 1),
    ("bz", 2, 1), ("ax2",), ("bzx", 2), ("bz", 2, -1), ("bx", 1), ("br", 0), ("ar", 0), ("xer",),
    ("az", 1, 1), ("az", -1, 1), ("bz", 3, 1), ("az", 2, 1), ("ar", 1), ("bx", 2), ("bzx", 3), ("az", 0, 2),
    ("az", 1, 2), ("xlo",), ("az", -1, 2), ("t", 1), ("bzx", 4), ("az", 2, 2), ("br", 1), ("az", 0, 3),
    ("ar", 2), ("bx", 3), ("f", 0), ("az", 1, 3), ("br", 2), ("az", -1, 3), ("f", 1), ("bx", 4), ("az", 2, 3),
    ("t", 2), ("f", 2), ("ar", 3), ("br", 3), ("f2",), ("br", 4), ("az", 1, 4), ("az", -1, 4), ("az", 0, 4),
    ("az", 2, 4), ("ar", 4), ("f", 3), ("f", 4), ("e", 2), ("e", 0), ("e", 1), ("xlr",), ("e", -1), ("i", 3),
    ("i", 2), ("y1", 1), ("w", 4), ("w", 3), ("sz", 2, 3), ("sx", 4), ("w", 2), ("sz", 1, 3), ("sz", -1, 3),
    ("sx", 3), ("sz", 0, 3), ("i", 1), ("st", 4), ("sz", 2, 2), ("w", 1), ("sz", 1, 2), ("i", 0),
    ("sz", -1, 2), ("y1", 0), ("sx", 2), ("sz", 0, 2), ("y2", 1), ("st", 3), ("sb", 3), ("sz", 2, 1),
    ("l", 1), ("w", 0), ("sz", -1, 1), ("sz", 1, 1), ("l", 2), ("sx", 1), ("st", 2), ("sb", 2), ("at", 2),
    ("sz", 0, 1), ("y2", 0), ("at", 1), ("sx", 0), ("st", 1), ("sb", 1), ("at", -1), ("sa",), ("at", 0),
    ("yf", 1), ("st", 0), ("l", 0), ("fa",), ("fb",), ("yf", 0),
)


def sigmoid(v):
    return 0.5 * jnp.tanh(0.5 * v) + 0.5


def rows_of(k):
    return (k,) if k in (0, 4) else (k, -k)


def group_of(key):
    name = key[0]
    if name in ("xt", "d"):
        return (name,)
    if name == "xe":
        return (name, key[1])
    if name == "xl":
        return (name, min(key[1], 1))
    if name in ("ar", "br"):
        return ("row", abs(key[1]))
    if name == "bx" and key[2] > 0:
        return (name, abs(key[1]))
    if name == "bx":
        return ("bxr", abs(key[1]))
    if name == "bxr":
        return (name, abs(key[1]))
    if name == "sx":
        return (name, abs(key[1]), key[2])
    if name == "y":
        return (name, key[1], 2 if key[2] == 2 else 1)
    if name == "az" and key[2] == 3:
        return ("az", 3)
    if name == "sz" and key[2] == 1:
        return ("sz", abs(key[1]))
    if name in ("sz", "sa", "sb"):
        return key[:-2]
    return key[:-1]


def kernel(
    x_late, x_early, d_hidden, w_gate, w_up, gate_sum, up_sum,
    hidden_out, grad_out, gate_out, up_out,
    xe, xl, w, dh, sums, xt, xtp, d, pd, acc, s, ta, tb,
    a_stage, a_in, b_stage, b_in, part, y_stage, y_in, hid, grad, sized,
    send_sem, recv_sem, local_sem,
):
    fs = lax.axis_index("fs")
    y = lax.axis_index("tp")
    z, x, c = fs // (X * C), (fs // C) % X, fs % C

    def zk(k):
        return lax.rem(z + (k + Z), Z)

    def xk(k):
        return lax.rem(x + (k + X), X)

    def yk(k):
        return lax.rem(y + (k + Y), Y)

    def at(zz, xx, cc, yy):
        return {"fs": (zz * X + xx) * C + cc, "tp": yy}

    zp = {k: at(zk(k), x, c, y) for k in DIRS}
    xp = {k: at(z, xk(k), c, y) for k in DIRS}
    yp = {k: at(z, x, c, yk(k)) for k in DIRS}
    pal = at(z, x, 1 - c, y)

    local = {}

    def load(group, src, dst):
        into = local.setdefault(group, [len(local), 0, False])
        pltpu.make_async_copy(src, dst, local_sem.at[into[0]]).start()
        into[1] += bytes_of(src)

    def loaded(group):
        into = local[group]
        if not into[2]:
            into[2] = True
            taken(local_sem.at[into[0]], into[1])

    def bytes_of(ref):
        size = ref.dtype.itemsize
        for extent in ref.shape:
            size *= extent
        return size

    def taken(sem, size):
        ref = sized.at[pl.ds(0, size // 512)]
        pltpu.make_async_copy(ref, ref, sem).wait()

    def store(src, dst):
        load("out", src, dst)

    load("w", w_up, w.at[z, x, c, :, pl.ds(HID, HID)])
    load("w", w_gate, w.at[z, x, c, :, pl.ds(0, HID)])
    for h in range(2):
        load("xe", x_early.at[pl.ds(h * HALF, HALF)], xe.at[y, h])
    for h in range(2):
        load("xl", x_late.at[pl.ds(h * HALF, HALF)], xl.at[y, h])
    for i in range(Y):
        load("rest", d_hidden.at[pl.ds(i * ROWS, ROWS)], dh.at[i])
    load("rest", gate_sum, sums.at[:, pl.ds(0, HID)])
    load("rest", up_sum, sums.at[:, pl.ds(HID, HID)])

    with jax.named_scope("entry"):
        barrier = pltpu.get_barrier_semaphore()
        for peer in (*zp.values(), *xp.values(), *yp.values(), pal):
            pl.semaphore_signal(barrier, inc=1, device_id=peer, device_id_type=MESH)
        pl.semaphore_wait(barrier, 7)

    groups, links = {}, {}

    def send(key, src, dst, peer):
        group, link = group_of(key), id(peer)
        into = groups.setdefault(group, [len(groups), 0, False])
        out = links.setdefault(link, [len(links), 0])
        if into[2]:
            raise ValueError(key)
        pltpu.make_async_remote_copy(
            src_ref=src, dst_ref=dst, send_sem=send_sem.at[out[0]], recv_sem=recv_sem.at[into[0]],
            device_id=peer, device_id_type=MESH,
        ).start()
        into[1] += bytes_of(src)
        out[1] += bytes_of(src)

    def push(key, ref, peer):
        send(key, ref, ref, peer)

    def wait(*group):
        into = groups[group]
        if not into[2]:
            into[2] = True
            taken(recv_sem.at[into[0]], into[1])

    def half(k):
        return pl.ds(0, 16) if k > 0 else pl.ds(16, 16)

    ALL = pl.ds(0, SHARD)
    CA, CB = pl.ds(0, NA), pl.ds(NA, NB)

    def own():
        loaded("w")
        for p in (1, -1):
            for k in DIRS:
                push(("bz", 0, p, k), w.at[z, x, c, half(p * k), CB], zp[k])
        for k in DIRS:
            push(("ax", k), w.at[z, x, c, :, CA], xp[k])
        for p in (1, -1):
            for k in DIRS:
                push(("bx", 0, p, k), w.at[z, x, c, half(p * k), CB], xp[k])
        for k in DIRS:
            push(("az", 0, 0, k), w.at[z, x, c, :, CA], zp[k])
        loaded("xe")
        y_own("xe", xe)

    def y_own(name, ref):
        for i in range(2):
            for k in DIRS:
                h = i if k > 0 else 1 - i
                push((name, i, k), ref.at[y, h], yp[k])

    def y_relay(name, ref):
        wait(name, 0)
        for k in DIRS:
            push((name, 2, k), ref.at[yk(-k), 0 if k > 0 else 1], yp[k])

    def xl_own():
        loaded("xl")
        y_own("xl", xl)

    def turn(block):
        tokens = pl.ds(pl.multiple_of(block * ROWS, ROWS), ROWS)

        def step(zz, carry):
            span = pl.ds(pl.multiple_of(zz * TILE, TILE), TILE)
            value = xe[block, :, :, span].reshape(ROWS, TILE)
            xt[zz, :, :, :, tokens] = value.T.reshape(X, C, SHARD, ROWS)
            return carry

        lax.fori_loop(0, Z, step, 0)
        return tokens

    def turns(which):
        if which == 1:
            wait("xe", 1)
        if which == 2:
            wait("xe", 2)
        for k in (1, -1) if which == 1 else (which,):
            tokens = turn(yk(k))
            send(("xt", k), xt.at[:, :, 1 - c, :, tokens], xtp.at[:, :, :, tokens], pal)

    def ax1():
        wait("ax")
        for k in DIRS:
            push(("axr", k), w.at[z, xk(-k), c, half(k), CA], xp[k])

    def az0():
        wait("ax")
        for j in DIRS:
            for k in DIRS:
                push(("az", j, 0, k), w.at[z, xk(j), c, :, CA], zp[k])

    def ax2():
        wait("axr")
        for k in DIRS:
            push(("az", 2, 0, k), w.at[z, xk(2), c, :, CA], zp[k])

    def az(j, n):
        if n == 4:
            return
        wait("az", j, n - 1)
        if n < 4:
            for k in DIRS:
                rows = half(k) if n == 3 else ALL
                push(("az", j, n, k), w.at[zk(-k * n), xk(j), c, rows, CA], zp[k])

    def ar(n):
        if n == 4:
            wait("az", 3)
        for r in rows_of(n):
            push(("ar", r), w.at[zk(r), :, c, :, CA], pal)

    def bz(n, p):
        wait("bz", n - 1, p)
        for k in DIRS:
            push(("bz", n, p, k), w.at[zk(-k * n), x, c, half(p * k), CB], zp[k])

    def bzx(n):
        wait("bz", n - 1, 1)
        if n < 4:
            wait("bz", n - 1, -1)
        for p in (1, -1):
            for r in rows_of(n):
                for k in DIRS:
                    push(("bx", r, p, k), w.at[zk(r), x, c, half(p * k), CB], xp[k])

    def bx(n):
        wait("bx", n)
        for r in rows_of(n):
            for k in DIRS:
                push(("bxr", r, k), w.at[zk(r), xk(-k), c, half(k), CB], xp[k])

    def br(n):
        wait("bxr", n)
        for r in rows_of(n):
            push(("br", r), w.at[zk(r), :, c, :, CB], pal)

    def dot(a, b):
        return jnp.dot(a, b, preferred_element_type=F32)

    def rows_product(rows, blocks):
        spans = [pl.ds(pl.multiple_of(zk(r) * TILE, TILE), TILE) for r in rows]
        left = [[xe[yk(b), :, :, q].reshape(ROWS, TILE) for q in spans] for b in blocks]
        left = jnp.concatenate([jnp.concatenate(q, axis=1) for q in left], axis=0)
        right = jnp.concatenate([w[zk(r)].reshape(TILE, BOTH) for r in rows], axis=0)
        value = dot(left, right)
        return [(yk(b), value[i * ROWS : (i + 1) * ROWS]) for i, b in enumerate(blocks)]

    def f(n):
        wait("row", n)
        for block, piece in rows_product(rows_of(n), (0, 1, -1) if n < 3 else (0, 1, -1, 2)):
            acc[block] = piece if n == 0 else acc[block] + piece

    def f2():
        loaded("rest")
        for block, piece in rows_product((0, 1, -1, 2, -2), (2,)):
            acc[block] = piece

    def e(b):
        block = yk(b)
        gate, up = acc[block, :, :HID], acc[block, :, HID:]
        sig = sigmoid(gate)
        cot = dh[block].astype(F32) * sig
        d[block, :, :HID] = (cot * up * (1.0 + gate * (1.0 - sig))).astype(BF16)
        d[block, :, HID:] = (cot * gate).astype(BF16)
        send(("d", b), d.at[block], pd.at[block], pal)

    lates = []

    def late(t):
        if not lates:
            wait("xl", 1)
        lates.append(t)
        lo, hi = pl.ds(t * TILE, TILE), pl.ds(HID + t * TILE, TILE)
        left = xl[...].reshape(TOK, D)
        gate = dot(left, w[..., lo].reshape(D, TILE))
        up = dot(left, w[..., hi].reshape(D, TILE))
        hid[:, lo] = (gate * sigmoid(gate) * up).astype(BF16)
        store(hid.at[:, lo], hidden_out.at[:, lo])

    slots = {}

    def slot(kind, key):
        return slots.setdefault((kind, key), sum(1 for name in slots if name[0] == kind))

    def sent(kind, key, value, peer, rows=ALL, more=None, more_rows=None, part=0):
        stage, into = (a_stage, a_in) if kind == "a" else (b_stage, b_in)
        i = slot(kind, key)
        stage[i, rows] = value.astype(BF16)
        if more is not None:
            stage[i, more_rows] = more.astype(BF16)
            rows = ALL
        send((*key, part), stage.at[i, rows], into.at[i, rows], peer)

    def came(kind, *key):
        wait(*group_of((*key, 0)))
        ref = a_in if kind == "a" else b_in
        return ref, slot(kind, key)

    def wgrad(n):
        if n == 4:
            wait("d")
            wait("xt")
        rows = rows_of(n)
        mine = jnp.concatenate([xt[zk(r), :, c].reshape(X * SHARD, TOK) for r in rows], axis=0)
        theirs = jnp.concatenate([xtp[zk(r)].reshape(X * SHARD, TOK) for r in rows], axis=0)
        value = dot(mine, d[...].reshape(TOK, BOTH)) + dot(theirs, pd[...].reshape(TOK, BOTH))
        for i, r in enumerate(rows):
            s[zk(r)] = value[i * X * SHARD : (i + 1) * X * SHARD].reshape(X, SHARD, BOTH)
        for r in rows:
            for k in DIRS:
                sent("b", ("sx", r, 2, k), s[zk(r), xk(2), half(k), CB], xp[k], half(k))
        for r in rows:
            for k in DIRS:
                sent("b", ("sx", r, 1, k), s[zk(r), xk(k), half(-k), CB], xp[k], half(-k), part=1)
        if n == 4:
            for j in (2, 1, -1, 0):
                for k in DIRS:
                    sent("a", ("sz", j, 4, k), s[zk(4), xk(j), half(k), CA], zp[k], half(k))

    def onward(kind, before, key, own, peer, partly, k):
        ref, i = came(kind, *before)
        if partly is None:
            sent(kind, key, own(half(k)) + ref[i, half(k)].astype(F32), peer, half(k))
            return
        if partly:
            mine, rest = half(k), half(-k)
            sent(kind, key, own(mine) + ref[i, mine].astype(F32), peer, mine, own(rest), rest)
        else:
            sent(kind, key, own(ALL) + ref[i].astype(F32), peer)

    def sx(n):
        for r in rows_of(n):
            for k in DIRS:
                onward("b", ("sx", r, 2, k), ("sx", r, 1, k), lambda q: s[zk(r), xk(k), q, CB], xp[k], None, k)

    def both(kind, own, *key):
        value = own
        for k in DIRS:
            ref, i = came(kind, *key, k)
            value = value + ref[i].astype(F32)
        return value

    def st(n):
        for r in rows_of(n):
            tb[zk(r)] = both("b", s[zk(r), x, :, CB], "sx", r, 1)
        if n == 4:
            for k in DIRS:
                sent("b", ("sb", 4, k), tb[zk(4), half(k)], zp[k], half(k))

    def sb(n):
        for k in DIRS:
            onward("b", ("sb", n + 1, k), ("sb", n, k), lambda q: tb[zk(k * n), q], zp[k], n == 3, k)

    def fb():
        sums[:, CB] = sums[:, CB] + both("b", tb[z], "sb", 1)
        store(sums.at[:, pl.ds(NA, HID - NA)], gate_out.at[:, pl.ds(NA, HID - NA)])
        store(sums.at[:, pl.ds(HID, HID)], up_out)

    def sz(j, n):
        for k in DIRS:
            onward("a", ("sz", j, n + 1, k), ("sz", j, n, k), lambda q: s[zk(k * n), xk(j), q, CA], zp[k], n == 3, k)

    def at_x(j):
        ta[xk(j)] = both("a", s[z, xk(j), :, CA], "sz", j, 1)
        if j == 2:
            for k in DIRS:
                sent("a", ("sa", 2, k), ta[xk(2), half(k)], xp[k], half(k))

    def sa():
        for k in DIRS:
            onward("a", ("sa", 2, k), ("sa", 1, k), lambda q: ta[xk(k), q], xp[k], True, k)

    def fa():
        sums[:, CA] = sums[:, CA] + both("a", ta[x], "sa", 1)
        store(sums.at[:, CA], gate_out.at[:, CA])

    def igrad(n):
        span = pl.ds(n * 2 * TILE, 2 * TILE)
        weights = w[2 * n : 2 * n + 2].reshape(2 * TILE, BOTH)
        value = lax.dot_general(d[...].reshape(TOK, BOTH), weights, (((1,), (1,)), ((), ())), preferred_element_type=F32)
        part[..., span] = value.astype(BF16).reshape(Y, 2, HALF, 2 * TILE)

    def y_cols(h):
        return pl.ds(h * (D // 2), D // 2)

    def y1(h):
        for m, which in ((2, 2), (3, 1)):
            for k in DIRS:
                side = (0 if k > 0 else 1) if m == 2 else (1 if k > 0 else 0)
                i = 4 * h + 2 * (m - 2) + (0 if k > 0 else 1)
                send(("y", h, m, k), part.at[yk(which * k), side, :, y_cols(h)], y_in.at[i], yp[k])

    def y2(h):
        for k in DIRS:
            i = 0 if k > 0 else 1
            wait("y", h, 2)
            value = part[yk(k), i, :, y_cols(h)].astype(F32) + y_in[4 * h + i].astype(F32)
            y_stage[2 * h + i] = value.astype(BF16)
            send(("y", h, 1, k), y_stage.at[2 * h + i], y_in.at[8 + 2 * h + i], yp[k])

    def yf(h):
        wait("y", h, 1)
        for side in range(2):
            value = part[y, side, :, y_cols(h)].astype(F32)
            value = value + y_in[8 + 2 * h + side].astype(F32)
            value = value + y_in[4 * h + 2 + (1 - side)].astype(F32)
            grad[pl.ds(side * HALF, HALF), y_cols(h)] = value.astype(BF16)
        store(grad.at[:, y_cols(h)], grad_out.at[:, y_cols(h)])

    tasks = {
        "own": own, "t": turns, "xer": lambda: y_relay("xe", xe), "xlo": xl_own,
        "xlr": lambda: y_relay("xl", xl), "ax1": ax1, "az0": az0, "bzx": bzx, "ax2": ax2, "az": az, "ar": ar, "bz": bz, "bx": bx,
        "br": br, "f": f, "f2": f2, "e": e, "w": wgrad, "sx": sx, "st": st, "sb": sb, "fb": fb, "sz": sz,
        "at": at_x, "sa": sa, "fa": fa, "i": igrad, "y1": y1, "y2": y2, "yf": yf, "l": late,
    }
    for name, *args in ORDER:
        with jax.named_scope("_".join(map(str, (name, *args)))):
            tasks[name](*args)
    if len(groups) != GROUPS:
        raise ValueError(len(groups))
    with jax.named_scope("drain"):
        for i, size in links.values():
            taken(send_sem.at[i], size)
        loaded("out")


def finish(*refs):
    ins, outs, held, sems = refs[:4], refs[4:8], refs[8:12], refs[12]
    into = [pltpu.make_async_copy(a, b, sems.at[0, i]) for i, (a, b) in enumerate(zip(ins, held))]
    out = [pltpu.make_async_copy(a, b, sems.at[1, i]) for i, (a, b) in enumerate(zip(held, outs))]
    for copy in into:
        copy.start()
    for first, second in zip(into, out):
        first.wait()
        second.start()
    for copy in out:
        copy.wait()


def local(*args):
    any_space = pl.BlockSpec(memory_space=pl.ANY)
    vmem = pltpu.VMEM
    held = pl.pallas_call(
            kernel,
            out_shape=OUTS,
            in_specs=[any_space] * 7,
            out_specs=[any_space] * 4,
            scratch_shapes=[
                vmem((Y, 2, HALF, D), BF16),
                vmem((Y, 2, HALF, D), BF16),
                vmem((Z, X, C, SHARD, BOTH), BF16),
                vmem((Y, ROWS, HID), BF16),
                vmem((SHARD, BOTH), F32),
                vmem((Z, X, C, SHARD, TOK), BF16),
                vmem((Z, X, SHARD, TOK), BF16),
                vmem((Y, ROWS, BOTH), BF16),
                vmem((Y, ROWS, BOTH), BF16),
                vmem((Y, ROWS, BOTH), F32),
                vmem((Z, X, SHARD, BOTH), F32),
                vmem((X, SHARD, NA), F32),
                vmem((Z, SHARD, NB), F32),
                vmem((36, SHARD, NA), BF16),
                vmem((36, SHARD, NA), BF16),
                vmem((40, SHARD, NB), BF16),
                vmem((40, SHARD, NB), BF16),
                vmem((Y, 2, HALF, D), BF16),
                vmem((4, HALF, D // 2), BF16),
                vmem((12, HALF, D // 2), BF16),
                vmem((TOK, HID), BF16),
                vmem((ROWS, D), BF16),
                vmem((SIZED, 128), F32),
                pltpu.SemaphoreType.DMA((7,)),
                pltpu.SemaphoreType.DMA((GROUPS,)),
                pltpu.SemaphoreType.DMA((5,)),
            ],
            compiler_params=pltpu.CompilerParams(
                collective_id=0, has_side_effects=True, vmem_limit_bytes=VMEM_MIB * 1024 * 1024
            ),
            cost_estimate=pl.CostEstimate(flops=8 * TOK * D * BOTH, bytes_accessed=8 << 20, transcendentals=0),
            name="layer",
        )(*args)
    return tuple(
        pl.pallas_call(
            finish,
            out_shape=OUTS,
            in_specs=[any_space] * 4,
            out_specs=[any_space] * 4,
            scratch_shapes=[*(vmem(a.shape, a.dtype) for a in OUTS), pltpu.SemaphoreType.DMA((2, 4))],
            name="finish",
        )(*held)
    )


OUTS = (
    jax.ShapeDtypeStruct((TOK, HID), BF16),
    jax.ShapeDtypeStruct((ROWS, D), BF16),
    jax.ShapeDtypeStruct((SHARD, HID), F32),
    jax.ShapeDtypeStruct((SHARD, HID), F32),
)
VMEM_MIB = 60


def solution(mesh):
    return jax.shard_map(
        local,
        mesh=mesh,
        in_specs=(
            P(("fs", "tp"), None),
            P(("fs", "tp"), None),
            P("fs", "tp"),
            P("fs", "tp"),
            P("fs", "tp"),
            P("fs", "tp"),
            P("fs", "tp"),
        ),
        out_specs=(P("fs", "tp"), P(("fs", "tp"), None), P("fs", "tp"), P("fs", "tp")),
        check_vma=False,
    )
```

```python
import jax
import jax.numpy as jnp
from jax import lax
from jax.experimental import pallas as pl
from jax.experimental.pallas import tpu as pltpu
from jax.sharding import PartitionSpec as P

Z, X, C, Y = 8, 4, 2, 4
D, HID, ROWS, SHARD = 2048, 768, 128, 32
BOTH = 2 * HID
NA = 640
NB = BOTH - NA
TOK = ROWS * Y
HALF = ROWS // 2
TILE = 256
MESH = pl.DeviceIdType.MESH
F32, BF16 = jnp.float32, jnp.bfloat16
DIRS = (1, -1)
GROUPS, SIZED = 78, 11264
ORDER = (
    ("own",), ("bz", 1, 1), ("ax1",), ("bz", 1, -1), ("bx", 0), ("bzx", 1), ("az0",), ("t", 0), ("az", 0, 1),
    ("bz", 2, 1), ("ax2",), ("bzx", 2), ("bz", 2, -1), ("bx", 1), ("br", 0), ("ar", 0), ("xer",),
    ("az", 1, 1), ("az", -1, 1), ("bz", 3, 1), ("az", 2, 1), ("ar", 1), ("bx", 2), ("bzx", 3), ("az", 0, 2),
    ("az", 1, 2), ("xlo",), ("az", -1, 2), ("t", 1), ("bzx", 4), ("az", 2, 2), ("br", 1), ("az", 0, 3),
    ("ar", 2), ("bx", 3), ("f", 0), ("az", 1, 3), ("br", 2), ("az", -1, 3), ("f", 1), ("bx", 4), ("az", 2, 3),
    ("t", 2), ("f", 2), ("ar", 3), ("br", 3), ("f2",), ("br", 4), ("az", 1, 4), ("az", -1, 4), ("az", 0, 4),
    ("az", 2, 4), ("ar", 4), ("f", 3), ("f", 4), ("e", 2), ("e", 0), ("e", 1), ("xlr",), ("e", -1), ("i", 3),
    ("i", 2), ("y1", 1), ("w", 4), ("w", 3), ("sz", 2, 3), ("sx", 4), ("w", 2), ("sz", 1, 3), ("sz", -1, 3),
    ("sx", 3), ("sz", 0, 3), ("i", 1), ("st", 4), ("sz", 2, 2), ("w", 1), ("sz", 1, 2), ("i", 0),
    ("sz", -1, 2), ("y1", 0), ("sx", 2), ("sz", 0, 2), ("y2", 1), ("st", 3), ("sb", 3), ("sz", 2, 1),
    ("l", 1), ("w", 0), ("sz", -1, 1), ("sz", 1, 1), ("l", 2), ("sx", 1), ("st", 2), ("sb", 2), ("at", 2),
    ("sz", 0, 1), ("y2", 0), ("sx", 0), ("l", 0), ("at", 1), ("st", 1), ("sb", 1), ("at", -1), ("sa",),
    ("at", 0), ("yf", 1), ("st", 0), ("fa",), ("fb",), ("yf", 0),
)


def sigmoid(v):
    return 0.5 * jnp.tanh(0.5 * v) + 0.5


def rows_of(k):
    return (k,) if k in (0, 4) else (k, -k)


def group_of(key):
    name = key[0]
    if name in ("xt", "d"):
        return ("d",)
    if name == "xe":
        return (name, key[1])
    if name == "xl":
        return (name, min(key[1], 1))
    if name in ("ar", "br"):
        return ("row", abs(key[1]))
    if name == "bx" and key[2] > 0:
        return (name, abs(key[1]))
    if name == "bx":
        return ("bxr", abs(key[1]))
    if name == "bxr":
        return (name, abs(key[1]))
    if name == "sx":
        return (name, abs(key[1]), key[2])
    if name == "y":
        return (name, key[1], 2 if key[2] == 2 else 1)
    if name == "az" and key[2] == 3:
        return ("az", 3)
    if name == "sz" and key[2] == 1:
        return ("sz", abs(key[1]))
    if name in ("sz", "sa", "sb"):
        return key[:-2]
    return key[:-1]


def kernel(
    x_late, x_early, d_hidden, w_gate, w_up, gate_sum, up_sum,
    hidden_out, grad_out, gate_out, up_out,
    xe, xl, w, dh, sums, xt, xtp, d, pd, acc, s, ta, tb,
    a_stage, a_in, b_stage, b_in, part, y_stage, y_in, hid, grad, sized,
    send_sem, recv_sem, local_sem,
):
    fs = lax.axis_index("fs")
    y = lax.axis_index("tp")
    z, x, c = fs // (X * C), (fs // C) % X, fs % C

    def zk(k):
        return lax.rem(z + (k + Z), Z)

    def xk(k):
        return lax.rem(x + (k + X), X)

    def yk(k):
        return lax.rem(y + (k + Y), Y)

    def at(zz, xx, cc, yy):
        return {"fs": (zz * X + xx) * C + cc, "tp": yy}

    zp = {k: at(zk(k), x, c, y) for k in DIRS}
    xp = {k: at(z, xk(k), c, y) for k in DIRS}
    yp = {k: at(z, x, c, yk(k)) for k in DIRS}
    pal = at(z, x, 1 - c, y)

    local = {}

    def load(group, src, dst):
        into = local.setdefault(group, [len(local), 0, False])
        pltpu.make_async_copy(src, dst, local_sem.at[into[0]]).start()
        into[1] += bytes_of(src)

    def loaded(group):
        into = local[group]
        if not into[2]:
            into[2] = True
            taken(local_sem.at[into[0]], into[1])

    def bytes_of(ref):
        size = ref.dtype.itemsize
        for extent in ref.shape:
            size *= extent
        return size

    def taken(sem, size):
        ref = sized.at[pl.ds(0, size // 512)]
        pltpu.make_async_copy(ref, ref, sem).wait()

    def store(src, dst):
        load("out", src, dst)

    load("w", w_up, w.at[z, x, c, :, pl.ds(HID, HID)])
    load("w", w_gate, w.at[z, x, c, :, pl.ds(0, HID)])
    for h in range(2):
        load("xe", x_early.at[pl.ds(h * HALF, HALF)], xe.at[y, h])
    for h in range(2):
        load("xl", x_late.at[pl.ds(h * HALF, HALF)], xl.at[y, h])
    for i in range(Y):
        load("rest", d_hidden.at[pl.ds(i * ROWS, ROWS)], dh.at[i])
    load("rest", gate_sum, sums.at[:, pl.ds(0, HID)])
    load("rest", up_sum, sums.at[:, pl.ds(HID, HID)])

    with jax.named_scope("entry"):
        barrier = pltpu.get_barrier_semaphore()
        for peer in (*zp.values(), *xp.values(), *yp.values(), pal):
            pl.semaphore_signal(barrier, inc=1, device_id=peer, device_id_type=MESH)
        pl.semaphore_wait(barrier, 7)

    groups, links = {}, {}

    def send(key, src, dst, peer):
        group, link = group_of(key), id(peer)
        into = groups.setdefault(group, [len(groups), 0, False])
        out = links.setdefault(link, [len(links), 0])
        if into[2]:
            raise ValueError(key)
        pltpu.make_async_remote_copy(
            src_ref=src, dst_ref=dst, send_sem=send_sem.at[out[0]], recv_sem=recv_sem.at[into[0]],
            device_id=peer, device_id_type=MESH,
        ).start()
        into[1] += bytes_of(src)
        out[1] += bytes_of(src)

    def push(key, ref, peer):
        send(key, ref, ref, peer)

    def wait(*group):
        into = groups[group]
        if not into[2]:
            into[2] = True
            taken(recv_sem.at[into[0]], into[1])

    def half(k):
        return pl.ds(0, 16) if k > 0 else pl.ds(16, 16)

    ALL = pl.ds(0, SHARD)
    CA, CB = pl.ds(0, NA), pl.ds(NA, NB)

    def own():
        loaded("w")
        for p in (1, -1):
            for k in DIRS:
                push(("bz", 0, p, k), w.at[z, x, c, half(p * k), CB], zp[k])
        for k in DIRS:
            push(("ax", k), w.at[z, x, c, :, CA], xp[k])
        for p in (1, -1):
            for k in DIRS:
                push(("bx", 0, p, k), w.at[z, x, c, half(p * k), CB], xp[k])
        for k in DIRS:
            push(("az", 0, 0, k), w.at[z, x, c, :, CA], zp[k])
        loaded("xe")
        y_own("xe", xe)

    def y_own(name, ref):
        for i in range(2):
            for k in DIRS:
                h = i if k > 0 else 1 - i
                push((name, i, k), ref.at[y, h], yp[k])

    def y_relay(name, ref):
        wait(name, 0)
        for k in DIRS:
            push((name, 2, k), ref.at[yk(-k), 0 if k > 0 else 1], yp[k])

    def xl_own():
        loaded("xl")
        y_own("xl", xl)

    def turn(block):
        tokens = pl.ds(pl.multiple_of(block * ROWS, ROWS), ROWS)

        def step(zz, carry):
            span = pl.ds(pl.multiple_of(zz * TILE, TILE), TILE)
            value = xe[block, :, :, span].reshape(ROWS, TILE)
            xt[zz, :, :, :, tokens] = value.T.reshape(X, C, SHARD, ROWS)
            return carry

        lax.fori_loop(0, Z, step, 0)
        return tokens

    def turns(which):
        if which == 1:
            wait("xe", 1)
        if which == 2:
            wait("xe", 2)
        for k in (1, -1) if which == 1 else (which,):
            tokens = turn(yk(k))
            send(("xt", k), xt.at[:, :, 1 - c, :, tokens], xtp.at[:, :, :, tokens], pal)

    def ax1():
        wait("ax")
        for k in DIRS:
            push(("axr", k), w.at[z, xk(-k), c, half(k), CA], xp[k])

    def az0():
        wait("ax")
        for j in DIRS:
            for k in DIRS:
                push(("az", j, 0, k), w.at[z, xk(j), c, :, CA], zp[k])

    def ax2():
        wait("axr")
        for k in DIRS:
            push(("az", 2, 0, k), w.at[z, xk(2), c, :, CA], zp[k])

    def az(j, n):
        if n == 4:
            return
        wait("az", j, n - 1)
        if n < 4:
            for k in DIRS:
                rows = half(k) if n == 3 else ALL
                push(("az", j, n, k), w.at[zk(-k * n), xk(j), c, rows, CA], zp[k])

    def ar(n):
        if n == 4:
            wait("az", 3)
        for r in rows_of(n):
            push(("ar", r), w.at[zk(r), :, c, :, CA], pal)

    def bz(n, p):
        wait("bz", n - 1, p)
        for k in DIRS:
            push(("bz", n, p, k), w.at[zk(-k * n), x, c, half(p * k), CB], zp[k])

    def bzx(n):
        wait("bz", n - 1, 1)
        if n < 4:
            wait("bz", n - 1, -1)
        for p in (1, -1):
            for r in rows_of(n):
                for k in DIRS:
                    push(("bx", r, p, k), w.at[zk(r), x, c, half(p * k), CB], xp[k])

    def bx(n):
        wait("bx", n)
        for r in rows_of(n):
            for k in DIRS:
                push(("bxr", r, k), w.at[zk(r), xk(-k), c, half(k), CB], xp[k])

    def br(n):
        wait("bxr", n)
        for r in rows_of(n):
            push(("br", r), w.at[zk(r), :, c, :, CB], pal)

    def dot(a, b):
        return jnp.dot(a, b, preferred_element_type=F32)

    def rows_product(rows, blocks):
        spans = [pl.ds(pl.multiple_of(zk(r) * TILE, TILE), TILE) for r in rows]
        left = [[xe[yk(b), :, :, q].reshape(ROWS, TILE) for q in spans] for b in blocks]
        left = jnp.concatenate([jnp.concatenate(q, axis=1) for q in left], axis=0)
        right = jnp.concatenate([w[zk(r)].reshape(TILE, BOTH) for r in rows], axis=0)
        value = dot(left, right)
        return [(yk(b), value[i * ROWS : (i + 1) * ROWS]) for i, b in enumerate(blocks)]

    def f(n):
        wait("row", n)
        for block, piece in rows_product(rows_of(n), (0, 1, -1) if n < 3 else (0, 1, -1, 2)):
            acc[block] = piece if n == 0 else acc[block] + piece

    def f2():
        loaded("rest")
        for block, piece in rows_product((0, 1, -1, 2, -2), (2,)):
            acc[block] = piece

    def e(b):
        block = yk(b)
        gate, up = acc[block, :, :HID], acc[block, :, HID:]
        sig = sigmoid(gate)
        cot = dh[block].astype(F32) * sig
        d[block, :, :HID] = (cot * up * (1.0 + gate * (1.0 - sig))).astype(BF16)
        d[block, :, HID:] = (cot * gate).astype(BF16)
        send(("d", b), d.at[block], pd.at[block], pal)

    lates = []

    def late(t):
        if not lates:
            wait("xl", 1)
        lates.append(t)
        lo, hi = pl.ds(t * TILE, TILE), pl.ds(HID + t * TILE, TILE)
        left = xl[...].reshape(TOK, D)
        gate = dot(left, w[..., lo].reshape(D, TILE))
        up = dot(left, w[..., hi].reshape(D, TILE))
        hid[:, lo] = (gate * sigmoid(gate) * up).astype(BF16)
        store(hid.at[:, lo], hidden_out.at[:, lo])

    slots = {}

    def slot(kind, key):
        return slots.setdefault((kind, key), sum(1 for name in slots if name[0] == kind))

    def sent(kind, key, value, peer, rows=ALL, more=None, more_rows=None, part=0):
        stage, into = (a_stage, a_in) if kind == "a" else (b_stage, b_in)
        i = slot(kind, key)
        stage[i, rows] = value.astype(BF16)
        if more is not None:
            stage[i, more_rows] = more.astype(BF16)
            rows = ALL
        send((*key, part), stage.at[i, rows], into.at[i, rows], peer)

    def came(kind, *key):
        wait(*group_of((*key, 0)))
        ref = a_in if kind == "a" else b_in
        return ref, slot(kind, key)

    def wgrad(n):
        if n == 4:
            wait("d")
        rows = rows_of(n)
        mine = jnp.concatenate([xt[zk(r), :, c].reshape(X * SHARD, TOK) for r in rows], axis=0)
        theirs = jnp.concatenate([xtp[zk(r)].reshape(X * SHARD, TOK) for r in rows], axis=0)
        value = dot(mine, d[...].reshape(TOK, BOTH)) + dot(theirs, pd[...].reshape(TOK, BOTH))
        for i, r in enumerate(rows):
            s[zk(r)] = value[i * X * SHARD : (i + 1) * X * SHARD].reshape(X, SHARD, BOTH)
        for r in rows:
            for k in DIRS:
                sent("b", ("sx", r, 2, k), s[zk(r), xk(2), half(k), CB], xp[k], half(k))
        for r in rows:
            for k in DIRS:
                sent("b", ("sx", r, 1, k), s[zk(r), xk(k), half(-k), CB], xp[k], half(-k), part=1)
        if n == 4:
            for j in (2, 1, -1, 0):
                for k in DIRS:
                    sent("a", ("sz", j, 4, k), s[zk(4), xk(j), half(k), CA], zp[k], half(k))

    def onward(kind, before, key, own, peer, partly, k):
        ref, i = came(kind, *before)
        if partly is None:
            sent(kind, key, own(half(k)) + ref[i, half(k)].astype(F32), peer, half(k))
            return
        if partly:
            mine, rest = half(k), half(-k)
            sent(kind, key, own(mine) + ref[i, mine].astype(F32), peer, mine, own(rest), rest)
        else:
            sent(kind, key, own(ALL) + ref[i].astype(F32), peer)

    def sx(n):
        for r in rows_of(n):
            for k in DIRS:
                onward("b", ("sx", r, 2, k), ("sx", r, 1, k), lambda q: s[zk(r), xk(k), q, CB], xp[k], None, k)

    def both(kind, own, *key):
        value = own
        for k in DIRS:
            ref, i = came(kind, *key, k)
            value = value + ref[i].astype(F32)
        return value

    def st(n):
        for r in rows_of(n):
            tb[zk(r)] = both("b", s[zk(r), x, :, CB], "sx", r, 1)
        if n == 4:
            for k in DIRS:
                sent("b", ("sb", 4, k), tb[zk(4), half(k)], zp[k], half(k))

    def sb(n):
        for k in DIRS:
            onward("b", ("sb", n + 1, k), ("sb", n, k), lambda q: tb[zk(k * n), q], zp[k], n == 3, k)

    def fb():
        sums[:, CB] = sums[:, CB] + both("b", tb[z], "sb", 1)
        store(sums.at[:, pl.ds(NA, HID - NA)], gate_out.at[:, pl.ds(NA, HID - NA)])
        store(sums.at[:, pl.ds(HID, HID)], up_out)

    def sz(j, n):
        for k in DIRS:
            onward("a", ("sz", j, n + 1, k), ("sz", j, n, k), lambda q: s[zk(k * n), xk(j), q, CA], zp[k], n == 3, k)

    def at_x(j):
        ta[xk(j)] = both("a", s[z, xk(j), :, CA], "sz", j, 1)
        if j == 2:
            for k in DIRS:
                sent("a", ("sa", 2, k), ta[xk(2), half(k)], xp[k], half(k))

    def sa():
        for k in DIRS:
            onward("a", ("sa", 2, k), ("sa", 1, k), lambda q: ta[xk(k), q], xp[k], True, k)

    def fa():
        sums[:, CA] = sums[:, CA] + both("a", ta[x], "sa", 1)
        store(sums.at[:, CA], gate_out.at[:, CA])

    def igrad(n):
        span = pl.ds(n * 2 * TILE, 2 * TILE)
        weights = w[2 * n : 2 * n + 2].reshape(2 * TILE, BOTH)
        value = lax.dot_general(d[...].reshape(TOK, BOTH), weights, (((1,), (1,)), ((), ())), preferred_element_type=F32)
        part[..., span] = value.astype(BF16).reshape(Y, 2, HALF, 2 * TILE)

    def y_cols(h):
        return pl.ds(h * (D // 2), D // 2)

    def y1(h):
        for m, which in ((2, 2), (3, 1)):
            for k in DIRS:
                side = (0 if k > 0 else 1) if m == 2 else (1 if k > 0 else 0)
                i = 4 * h + 2 * (m - 2) + (0 if k > 0 else 1)
                send(("y", h, m, k), part.at[yk(which * k), side, :, y_cols(h)], y_in.at[i], yp[k])

    def y2(h):
        for k in DIRS:
            i = 0 if k > 0 else 1
            wait("y", h, 2)
            value = part[yk(k), i, :, y_cols(h)].astype(F32) + y_in[4 * h + i].astype(F32)
            y_stage[2 * h + i] = value.astype(BF16)
            send(("y", h, 1, k), y_stage.at[2 * h + i], y_in.at[8 + 2 * h + i], yp[k])

    def yf(h):
        wait("y", h, 1)
        for side in range(2):
            value = part[y, side, :, y_cols(h)].astype(F32)
            value = value + y_in[8 + 2 * h + side].astype(F32)
            value = value + y_in[4 * h + 2 + (1 - side)].astype(F32)
            grad[pl.ds(side * HALF, HALF), y_cols(h)] = value.astype(BF16)
        store(grad.at[:, y_cols(h)], grad_out.at[:, y_cols(h)])

    tasks = {
        "own": own, "t": turns, "xer": lambda: y_relay("xe", xe), "xlo": xl_own,
        "xlr": lambda: y_relay("xl", xl), "ax1": ax1, "az0": az0, "bzx": bzx, "ax2": ax2, "az": az, "ar": ar, "bz": bz, "bx": bx,
        "br": br, "f": f, "f2": f2, "e": e, "w": wgrad, "sx": sx, "st": st, "sb": sb, "fb": fb, "sz": sz,
        "at": at_x, "sa": sa, "fa": fa, "i": igrad, "y1": y1, "y2": y2, "yf": yf, "l": late,
    }
    for name, *args in ORDER:
        with jax.named_scope("_".join(map(str, (name, *args)))):
            tasks[name](*args)
    if len(groups) != GROUPS:
        raise ValueError(len(groups))
    with jax.named_scope("drain"):
        for i, size in links.values():
            taken(send_sem.at[i], size)
        loaded("out")


def finish(*refs):
    ins, outs, held, sems = refs[:4], refs[4:8], refs[8:12], refs[12]
    into = [pltpu.make_async_copy(a, b, sems.at[0, i]) for i, (a, b) in enumerate(zip(ins, held))]
    out = [pltpu.make_async_copy(a, b, sems.at[1, i]) for i, (a, b) in enumerate(zip(held, outs))]
    for copy in into:
        copy.start()
    for first, second in zip(into, out):
        first.wait()
        second.start()
    for copy in out:
        copy.wait()


def local(*args):
    any_space = pl.BlockSpec(memory_space=pl.ANY)
    vmem = pltpu.VMEM
    held = pl.pallas_call(
            kernel,
            out_shape=OUTS,
            in_specs=[any_space] * 7,
            out_specs=[any_space] * 4,
            scratch_shapes=[
                vmem((Y, 2, HALF, D), BF16),
                vmem((Y, 2, HALF, D), BF16),
                vmem((Z, X, C, SHARD, BOTH), BF16),
                vmem((Y, ROWS, HID), BF16),
                vmem((SHARD, BOTH), F32),
                vmem((Z, X, C, SHARD, TOK), BF16),
                vmem((Z, X, SHARD, TOK), BF16),
                vmem((Y, ROWS, BOTH), BF16),
                vmem((Y, ROWS, BOTH), BF16),
                vmem((Y, ROWS, BOTH), F32),
                vmem((Z, X, SHARD, BOTH), F32),
                vmem((X, SHARD, NA), F32),
                vmem((Z, SHARD, NB), F32),
                vmem((36, SHARD, NA), BF16),
                vmem((36, SHARD, NA), BF16),
                vmem((40, SHARD, NB), BF16),
                vmem((40, SHARD, NB), BF16),
                vmem((Y, 2, HALF, D), BF16),
                vmem((4, HALF, D // 2), BF16),
                vmem((12, HALF, D // 2), BF16),
                vmem((TOK, HID), BF16),
                vmem((ROWS, D), BF16),
                vmem((SIZED, 128), F32),
                pltpu.SemaphoreType.DMA((7,)),
                pltpu.SemaphoreType.DMA((GROUPS,)),
                pltpu.SemaphoreType.DMA((5,)),
            ],
            compiler_params=pltpu.CompilerParams(
                collective_id=0, has_side_effects=True, vmem_limit_bytes=VMEM_MIB * 1024 * 1024
            ),
            cost_estimate=pl.CostEstimate(flops=8 * TOK * D * BOTH, bytes_accessed=8 << 20, transcendentals=0),
            name="layer",
        )(*args)
    return tuple(
        pl.pallas_call(
            finish,
            out_shape=OUTS,
            in_specs=[any_space] * 4,
            out_specs=[any_space] * 4,
            scratch_shapes=[*(vmem(a.shape, a.dtype) for a in OUTS), pltpu.SemaphoreType.DMA((2, 4))],
            name="finish",
        )(*held)
    )


OUTS = (
    jax.ShapeDtypeStruct((TOK, HID), BF16),
    jax.ShapeDtypeStruct((ROWS, D), BF16),
    jax.ShapeDtypeStruct((SHARD, HID), F32),
    jax.ShapeDtypeStruct((SHARD, HID), F32),
)
VMEM_MIB = 60


def solution(mesh):
    return jax.shard_map(
        local,
        mesh=mesh,
        in_specs=(
            P(("fs", "tp"), None),
            P(("fs", "tp"), None),
            P("fs", "tp"),
            P("fs", "tp"),
            P("fs", "tp"),
            P("fs", "tp"),
            P("fs", "tp"),
        ),
        out_specs=(P("fs", "tp"), P(("fs", "tp"), None), P("fs", "tp"), P("fs", "tp")),
        check_vma=False,
    )
```
